128 devices in a mesh: sp: 64 (over z, y, x), tp: 2 (over core).
Axes of the slice: x: 4, y: 4, z: 4, core: 2. Of those that a mesh axis runs over, the one named last changes fastest.
Arguments:
- ssm_input: bfloat16 [16384, 1024], P('sp', 'tp'), may hold values from -6 to 6
- lam_real: float32 [64, 64], P('tp'), may hold values from -0.034 to -5.4931641e-06, as said below
- lam_imag: float32 [64, 64], P('tp'), may hold values from -3 to 3, as said below
- state_in: float32 [2, 64, 16, 64], P(None, 'tp'), may hold values from -2 to 2
- read_out: float32 [64, 128, 16], P('tp'), may hold values from -0.5 to 0.5
- channel_skip: float32 [1024], P('tp'), may hold values from -3 to 3
- glu_weight: bfloat16 [1024, 1024], replicated, may hold values from -0.1875 to 0.1875
- out_weight: bfloat16 [1024, 2048], replicated, may hold values from -0.375 to 0.375
- residual: bfloat16 [16384, 2048], P(('sp', 'tp')), may hold values from -6 to 6
- norm_gain: float32 [2048], replicated, may hold values from 0.1 to 1.9
- expert_ids: int32 [16384, 2], P(('sp', 'tp')), may hold values from 0 to 127, as said below
- route_weight: float32 [16384, 2], P(('sp', 'tp')), may hold values from 0.25 to 1
- expert_gate: bfloat16 [128, 2048, 512], P(('sp', 'tp')), may hold values from -0.125 to 0.125
- expert_up: bfloat16 [128, 2048, 512], P(('sp', 'tp')), may hold values from -0.125 to 0.125
- expert_down: bfloat16 [128, 512, 2048], P(('sp', 'tp')), may hold values from -0.25 to 0.25
Outputs:
- layer_out: bfloat16 [16384, 2048], P(('sp', 'tp'))
The draws below stay inside these ranges and needn't reach their ends.
Inputs may be any that keep to these rules, and one draw needn't show every extreme that they name: `lam_real`: strictly negative. `lam_imag`: magnitude at least 0.5. `expert_ids`: A token's two experts differ and lie in the same group of 32 consecutive experts. Among the 128 rows of one device (aligned blocks) no expert is named more than 4 times, and some expert exactly 4 times; every expert is named in every such block.
All inputs are finite; a program needn't handle non-finite values.
Results may differ from the reference program's by a relative error of at most 0.006.
Values may be sent and summed in bfloat16 or wider, within the bound.
A program may use at most 128 MiB of HBM per device.

```python
import jax
import jax.numpy as jnp
import numpy as np
from jax import lax

D = 2048
GROUP_CH = 16
SSMG = 64
STATE = 64
SSMW = 1024
FF = 512
GROUPS = 4
EXPERTS = 128
ROWS_SP = 256
DEV_ROWS = 128
CAP = 4
TOKENS = 16384
N_SP = 64
N_TP = 2


def ssm_modes(key):
    base = jax.random.fold_in(key, 7)
    keys = jax.random.split(base, 5)
    share = 0.5
    slow_mask = jax.random.uniform(keys[0], (SSMG, STATE), jnp.float32) < share
    slow_rate = jax.random.uniform(keys[1], (SSMG, STATE), jnp.float32, 0.1, 1.0) / TOKENS
    fast_rate = jnp.exp(jax.random.uniform(keys[2], (SSMG, STATE), jnp.float32, jnp.log(0.01), jnp.log(0.033)))
    lam_real = -jnp.where(slow_mask, slow_rate, fast_rate)
    turn = jax.random.uniform(keys[3], (SSMG, STATE), jnp.float32, 0.5, 3.0)
    signs = jnp.where(jax.random.uniform(keys[4], (SSMG, STATE), jnp.float32) < 0.5, -1.0, 1.0)
    return (lam_real, turn * signs)


def draw_lam_real(key, part):
    return ssm_modes(key)[0].astype(jnp.float32)


def draw_lam_imag(key, part):
    return ssm_modes(key)[1].astype(jnp.float32)


def draw_state_in(key, part):
    lam_real, lam_imag = ssm_modes(key)
    magnitude = jnp.exp(lam_real)
    numer_re = magnitude * jnp.cos(lam_imag) - 1.0
    numer_im = magnitude * jnp.sin(lam_imag)
    hold_size = jnp.sqrt((numer_re * numer_re + numer_im * numer_im) / (lam_real * lam_real + lam_imag * lam_imag))
    spread = jnp.sqrt((1.0 - jnp.exp(2.0 * lam_real)) / (2.0 * GROUP_CH)) / hold_size
    noise = jnp.clip(jax.random.normal(jax.random.fold_in(key, 9), (2, SSMG, GROUP_CH, STATE), jnp.float32), -4.0, 4.0)
    return (noise * spread[None, :, None, :]).astype(jnp.float32)


def draw_expert_ids(key, part):
    block_count = TOKENS // DEV_ROWS
    per_group = EXPERTS // GROUPS
    shares = np.array([DEV_ROWS // 2, DEV_ROWS // 4, DEV_ROWS // 8, DEV_ROWS // 8])
    share_of = np.repeat(np.arange(4), shares)
    starts = np.concatenate([np.zeros(1, np.int64), np.cumsum(shares)[:-1]])
    rank_in = jnp.asarray(np.arange(DEV_ROWS) - starts[share_of], jnp.int32)
    share_index = jnp.asarray(share_of, jnp.int32)
    base = jax.random.fold_in(key, 13)

    def member_order(member_key):
        return jax.random.permutation(member_key, per_group)

    def one_block(block_key):
        keys = jax.random.split(block_key, 3)
        group_order = jax.random.permutation(keys[0], GROUPS).astype(jnp.int32)
        members = jax.vmap(member_order)(jax.random.split(keys[1], GROUPS)).astype(jnp.int32)
        chosen = group_order[share_index]
        first_pick = members[chosen, 2 * rank_in % per_group]
        second_pick = members[chosen, (2 * rank_in + 1) % per_group]
        pairs = jnp.stack([chosen * per_group + first_pick, chosen * per_group + second_pick], axis=1)
        shuffle = jax.random.permutation(keys[2], DEV_ROWS)
        return pairs[shuffle]
    return jax.vmap(one_block)(jax.random.split(base, block_count)).reshape(TOKENS, 2).astype(jnp.int32)


def level_of(rng, extent, shards, least, high):
    factor_of, own = 1.0, jax.random.fold_in(rng, 6)
    for dim, blocks in shards:
        heights = jnp.exp(jax.random.uniform(jax.random.fold_in(own, dim), (blocks,), jnp.float32, least / len(shards), high / len(shards)))
        factor_of = factor_of * jnp.repeat(heights, extent[dim] // blocks).reshape([-1 if axis == dim else 1 for axis in range(len(extent))])
    return factor_of


def normal_values(rng, shape, scale, limit, shards=(), kind=jnp.bfloat16):
    level = level_of(rng, shape, shards, -0.22, 0.18) if shards else 1.0
    entries = jax.random.normal(rng, shape, jnp.float32) * scale * level
    return jnp.minimum(jnp.maximum(entries, -limit), limit).astype(kind)


def setup_inputs(seed: int = 0) -> dict:
    splits = jax.random.split(jax.random.key(seed), 16)
    return {
        "ssm_input": normal_values(splits[0], (TOKENS, SSMW), 1.0, 6.0, ((0, 64), (1, 2))),
        "lam_real": draw_lam_real(jax.random.fold_in(splits[15], 71), 0),
        "lam_imag": draw_lam_imag(jax.random.fold_in(splits[15], 71), 0),
        "state_in": draw_state_in(jax.random.fold_in(splits[15], 71), 0),
        "read_out": normal_values(splits[4], (SSMG, 2 * STATE, GROUP_CH), (2 * STATE) ** -0.5, 0.5, ((0, 2),), jnp.float32),
        "channel_skip": normal_values(splits[5], (SSMW,), 0.5, 3.0, ((0, 2),), jnp.float32),
        "glu_weight": normal_values(splits[6], (SSMW, SSMW), SSMW ** -0.5, 0.1875),
        "out_weight": normal_values(splits[7], (SSMW, D), (SSMW // 4) ** -0.5, 0.375),
        "residual": normal_values(splits[8], (TOKENS, D), 1.0, 6.0, ((0, 128),)),
        "norm_gain": jnp.clip(1.0 + 0.18 * jax.random.normal(splits[9], (D,), jnp.float32), 0.1, 1.9),
        "expert_ids": draw_expert_ids(jax.random.fold_in(splits[15], 71), 0),
        "route_weight": jnp.clip(0.25 + 0.75 * jax.random.uniform(splits[11], (TOKENS, 2), jnp.float32) ** level_of(splits[11], (TOKENS, 2), ((0, 128),), -0.2, 0.2), 0.25, 1.0),
        "expert_gate": normal_values(splits[12], (EXPERTS, D, FF), D ** -0.5, 0.125, ((0, 128),)),
        "expert_up": normal_values(splits[13], (EXPERTS, D, FF), D ** -0.5, 0.125, ((0, 128),)),
        "expert_down": normal_values(splits[14], (EXPERTS, FF, D), FF ** -0.5, 0.25, ((0, 128),)),
    }


EPSILON = 1e-06

def discretize(lam_real, lam_imag, state_in):
    magnitude = jnp.exp(lam_real)
    decay_re = magnitude * jnp.cos(lam_imag)
    decay_im = magnitude * jnp.sin(lam_imag)
    numer_re = decay_re - 1.0
    denom = lam_real * lam_real + lam_imag * lam_imag
    hold_re = ((numer_re * lam_real + decay_im * lam_imag) / denom)[:, None, :]
    hold_im = ((decay_im * lam_real - numer_re * lam_imag) / denom)[:, None, :]
    drive_re = hold_re * state_in[0] - hold_im * state_in[1]
    drive_im = hold_re * state_in[1] + hold_im * state_in[0]
    drive = jnp.concatenate([drive_re, drive_im], axis=-1).astype(jnp.bfloat16)
    return (decay_re, decay_im, drive)

def powers(lam_real, lam_imag, exponent):
    magnitude = jnp.exp(exponent[:, None, None] * lam_real[None])
    angle = exponent[:, None, None] * lam_imag[None]
    return (magnitude * jnp.cos(angle), magnitude * jnp.sin(angle))

def combine_steps(earlier, later):
    return (later[0] * earlier[0] - later[1] * earlier[1], later[0] * earlier[1] + later[1] * earlier[0], later[0] * earlier[2] - later[1] * earlier[3] + later[2], later[0] * earlier[3] + later[1] * earlier[2] + later[3])

def block_states(push_re, push_im, decay_re, decay_im):
    shape_in = push_re.shape
    flat_re = push_re.reshape(shape_in[0], -1)
    flat_im = push_im.reshape(shape_in[0], -1)
    scale_re = jnp.broadcast_to(decay_re.reshape(1, -1), flat_re.shape)
    scale_im = jnp.broadcast_to(decay_im.reshape(1, -1), flat_im.shape)
    result = lax.associative_scan(combine_steps, (scale_re, scale_im, flat_re, flat_im), axis=0)
    return (result[2].reshape(shape_in), result[3].reshape(shape_in))

def readout(part_re, part_im, read_out):
    stacked = jnp.concatenate([part_re, part_im], axis=-1)
    return jnp.einsum('tgq,gqm->tgm', stacked, read_out, precision=lax.Precision.HIGHEST)

def reference(ssm_input, lam_real, lam_imag, state_in, read_out, channel_skip, glu_weight, out_weight, residual, norm_gain, expert_ids, route_weight, expert_gate, expert_up, expert_down):
    decay_re, decay_im, drive = discretize(lam_real, lam_imag, state_in)
    block_count = TOKENS // ROWS_SP
    inputs = ssm_input.reshape(block_count, ROWS_SP, SSMG, GROUP_CH)
    skips = channel_skip.reshape(SSMG, GROUP_CH)
    ahead_re, ahead_im = powers(lam_real, lam_imag, jnp.arange(1, ROWS_SP + 1).astype(jnp.float32))

    def one_block(carry, block_input):
        carry_re, carry_im = carry
        pushed = jnp.einsum('tgm,gmp->tgp', block_input.astype(jnp.float32), drive.astype(jnp.float32), precision=lax.Precision.HIGHEST)
        state_re, state_im = block_states(pushed[..., :STATE], pushed[..., STATE:], decay_re, decay_im)
        state_re = state_re + ahead_re * carry_re - ahead_im * carry_im
        state_im = state_im + ahead_re * carry_im + ahead_im * carry_re
        read = readout(state_re, state_im, read_out)
        pre = jax.nn.gelu(read + skips * block_input.astype(jnp.float32)).astype(jnp.bfloat16)
        return ((state_re[-1], state_im[-1]), pre)
    start = (jnp.zeros((SSMG, STATE), jnp.float32), jnp.zeros((SSMG, STATE), jnp.float32))
    _, pre = lax.scan(one_block, start, inputs)
    pre = pre.reshape(TOKENS, SSMW)
    gate_lin = jnp.dot(pre, glu_weight, preferred_element_type=jnp.float32)
    gated = (pre.astype(jnp.float32) * jax.nn.sigmoid(gate_lin)).astype(jnp.bfloat16)
    mixed = residual.astype(jnp.float32) + jnp.dot(gated, out_weight, preferred_element_type=jnp.float32)
    normed = (mixed * lax.rsqrt(lax.optimization_barrier(jnp.mean(mixed * mixed, axis=-1, keepdims=True)) + EPSILON) * norm_gain).astype(jnp.bfloat16)
    device_count = N_SP * N_TP
    route_count = expert_ids.shape[1]
    slot_ids = expert_ids.reshape(device_count, DEV_ROWS * route_count)
    onehot = (slot_ids[:, :, None] == jnp.arange(EXPERTS, dtype=jnp.int32)[None, None, :]).astype(jnp.int32)
    rank = lax.optimization_barrier(jnp.sum(jnp.cumsum(onehot, axis=1) * onehot, axis=2)) - 1
    position = ((slot_ids * device_count + jnp.arange(device_count, dtype=jnp.int32)[:, None]) * CAP + rank).reshape(-1).astype(jnp.int32)
    slot_total = EXPERTS * device_count * CAP
    token_of = jnp.zeros((slot_total,), jnp.int32).at[position].set((jnp.arange(TOKENS * route_count) // route_count).astype(jnp.int32))
    weight_of = jnp.zeros((slot_total,), jnp.float32).at[position].set(route_weight.reshape(-1))
    per_expert = device_count * CAP

    def one_expert(expert, accum):
        start_at = (expert * per_expert).astype(jnp.int32)
        chosen = lax.dynamic_slice_in_dim(token_of, start_at, per_expert)
        weights = lax.dynamic_slice_in_dim(weight_of, start_at, per_expert)
        rows_in = normed[chosen]
        gate_part = jnp.dot(rows_in, expert_gate[expert], preferred_element_type=jnp.float32)
        up_part = jnp.dot(rows_in, expert_up[expert], preferred_element_type=jnp.float32)
        hidden = (jax.nn.silu(gate_part) * up_part).astype(jnp.bfloat16)
        answer = jnp.dot(hidden, expert_down[expert], preferred_element_type=jnp.float32).astype(jnp.bfloat16)
        return accum.at[chosen].add(answer.astype(jnp.float32) * weights[:, None])
    accum = lax.fori_loop(0, EXPERTS, one_expert, jnp.zeros((TOKENS, D), jnp.float32))
    return (mixed + accum).astype(jnp.bfloat16)
```

```python
import functools

import jax
import jax.numpy as jnp
from jax import lax
from jax.experimental import pallas as pl
from jax.experimental.pallas import tpu as pltpu
from jax.sharding import PartitionSpec as P

EPSILON = 1e-06
F32 = jnp.float32
BF16 = jnp.bfloat16
MESH = pl.DeviceIdType.MESH
SEG = 8
STEPS = 32
CHUNKS = 4
PER_CHUNK = 16


def dot(a, b):
    return jnp.dot(a, b, preferred_element_type=F32)


def iota(shape, dim):
    return lax.broadcasted_iota(jnp.int32, shape, dim)


def complex_mul(a, b):
    return a[0] * b[0] - a[1] * b[1], a[0] * b[1] + a[1] * b[0]


def complex_fma(a, b, c):
    return a[0] * b[0] - a[1] * b[1] + c[0], a[0] * b[1] + a[1] * b[0] + c[1]


def power(lam_real, lam_imag, exponent):
    magnitude = jnp.exp(exponent * lam_real)
    angle = exponent * lam_imag
    turns = jnp.floor(angle * 0.15915494309189535 + 0.5)
    angle = (angle - turns * 6.28125) - turns * 0.0019353071795864769
    return magnitude * jnp.cos(angle), magnitude * jnp.sin(angle)


def lanes_of(rows):
    return jnp.concatenate([rows[i : i + 1, :] for i in range(rows.shape[0])], axis=1)


def body(
    u_ref, lr_ref, li_ref, in_ref, ro_ref, skip_ref, gain_ref, meta_ref,
    glu_hbm, outw_hbm, res_hbm, wg_hbm, wu_hbm, wd_hbm,
    o_ref,
    glu, outw, res, wg, wu, wd, meta2,
    push, edge, fin, xbuf, ybuf, line, st, cblk, hot, comb,
    pre, mixed, normed, send, recv, ans, ret, part_out, part_in,
    hsem, xs, xr, ys, yr, psend, precv, ssem, rsem, asem, bsem,
):
    c = lax.axis_index("sp")
    k = lax.axis_index("tp")
    other = 1 - k
    z, y, x = c // 16, (c // 4) % 4, c % 4
    ln = c // 4

    def chip_at(i, sign):
        dz, dy, dx = i // 16, (i // 4) % 4, i % 4
        return (
            ((z + sign * dz + 4) % 4) * 16 + ((y + sign * dy + 4) % 4) * 4 + (x + sign * dx + 4) % 4
        )

    loads = [
        pltpu.make_async_copy(glu_hbm, glu, hsem.at[0]),
        pltpu.make_async_copy(outw_hbm, outw, hsem.at[1]),
        pltpu.make_async_copy(res_hbm, res.at[k], hsem.at[2]),
        pltpu.make_async_copy(wg_hbm.at[0], wg, hsem.at[3]),
        pltpu.make_async_copy(wu_hbm.at[0], wu, hsem.at[4]),
        pltpu.make_async_copy(wd_hbm.at[0], wd, hsem.at[5]),
    ]
    for load in loads:
        load.start()

    barrier = pltpu.get_barrier_semaphore()
    pl.semaphore_signal(barrier, inc=1, device_id=(c, other), device_id_type=MESH)

    def greet(i, carry):
        pl.semaphore_signal(barrier, inc=1, device_id=(chip_at(i, 1), k), device_id_type=MESH)
        return carry

    lax.fori_loop(1, 64, greet, 0)

    lam_r, lam_i = lr_ref[...], li_ref[...]
    decay_re, decay_im = power(lam_r, lam_i, 1.0)
    numer_re = decay_re - 1.0
    denom = lam_r * lam_r + lam_i * lam_i
    hold_re = (numer_re * lam_r + decay_im * lam_i) / denom
    hold_im = (decay_im * lam_r - numer_re * lam_i) / denom
    hold_re = jnp.broadcast_to(hold_re[:, None, :], (32, 16, 64)).reshape(512, 64)
    hold_im = jnp.broadcast_to(hold_im[:, None, :], (32, 16, 64)).reshape(512, 64)
    drive = (
        (hold_re * in_ref[0] - hold_im * in_ref[1]).astype(BF16),
        (hold_re * in_ref[1] + hold_im * in_ref[0]).astype(BF16),
    )
    spread = (iota((64, 1024), 1) % 64 == iota((64, 1024), 0)).astype(F32).astype(BF16)
    own_block = iota((256, 1024), 0) // 16 == iota((256, 1024), 1) // 64
    row, col = iota((256, 256), 0), iota((256, 256), 1)
    order = (col == (row % SEG) * STEPS + row // SEG).astype(F32).astype(BF16)
    unorder = (row == (col % SEG) * STEPS + col // SEG).astype(F32).astype(BF16)
    ordered = dot(order, u_ref[...]).astype(BF16)
    for half in range(2):
        for part in range(2):
            block = dot(drive[part][256 * half : 256 * half + 256], spread)
            block = jnp.where(own_block, block, 0.0).astype(BF16)
            push[part, :, 1024 * half : 1024 * half + 1024] = dot(
                ordered[:, 256 * half : 256 * half + 256], block
            )

    dense_r, dense_i = meta_ref[8:24, :], meta_ref[24:40, :]
    p1 = power(dense_r, dense_i, 1.0)
    p32 = power(dense_r, dense_i, 32.0)
    p64 = power(dense_r, dense_i, 64.0)
    p128 = power(dense_r, dense_i, 128.0)
    q1 = power(dense_r, dense_i, 256.0)
    q2 = complex_mul(q1, q1)
    q3 = complex_mul(q2, q1)
    q4 = complex_mul(q2, q2)
    one = (jnp.ones_like(dense_r), jnp.zeros_like(dense_r))

    def segment_powers(j):
        def lane(v):
            return jnp.broadcast_to(lanes_of(v[4 * j : 4 * j + 4, :]), (8, 512))

        return [tuple(lane(v) for v in p) for p in (p1, p32, p64, p128)]

    seg = iota((8, 512), 0)
    for j in range(4):
        at = 512 * j
        d1, d32, d64, d128 = segment_powers(j)

        def step(i, h):
            rows = pl.ds(pl.multiple_of(i * 8, 8), 8)
            return complex_fma(d1, h, (push[0, rows, at : at + 512], push[1, rows, at : at + 512]))

        zero = jnp.zeros((8, 512), F32)
        h = lax.fori_loop(0, STEPS, step, (zero, zero), unroll=4)
        for d, p in ((1, d32), (2, d64), (4, d128)):
            moved = tuple(jnp.where(seg >= d, pltpu.roll(v, d, 0), 0.0) for v in h)
            h = complex_fma(p, moved, h)
        for part in range(2):
            edge[part, :, at : at + 512] = jnp.where(seg >= 1, pltpu.roll(h[part], 1, 0), 0.0)
            for n in range(4):
                fin[part, 4 * j + n : 4 * j + n + 1, :] = h[part][7:8, 128 * n : 128 * n + 128]

    pl.semaphore_wait(barrier, 64)

    def remote(src, dst, s, r, device):
        return pltpu.make_async_remote_copy(
            src_ref=src, dst_ref=dst, send_sem=s, recv_sem=r, device_id=device, device_id_type=MESH
        )

    along = [
        remote(fin, xbuf.at[d - 1], xs.at[d - 1], xr.at[d - 1], (c - x + (x + d) % 4, k))
        for d in (1, 2, 3)
    ]
    for copy in along:
        copy.start()
    meta_copy = remote(meta_ref.at[0:8], meta2, psend.at[0], precv.at[0], (c, other))
    meta_copy.start()
    res_copy = remote(res_hbm, res.at[k], psend.at[1], precv.at[1], (c, other))
    res_copy.start()

    narrow = (iota((16, 256), 1) % 16 == iota((16, 256), 0)).astype(F32).astype(BF16)
    own_read = iota((1024, 256), 0) // 64 == iota((1024, 256), 1) // 16
    for half in range(2):
        for part in range(2):
            piece = ro_ref[16 * half : 16 * half + 16, 64 * part : 64 * part + 64, :]
            piece = dot(piece.reshape(1024, 16).astype(BF16), narrow)
            cblk[half, 1024 * part : 1024 * part + 1024, :] = jnp.where(own_read, piece, 0.0).astype(BF16)

    for copy in along:
        copy.wait()

    def pick(n):
        return tuple(
            jnp.where(n == 0, a, jnp.where(n == 1, b, jnp.where(n == 2, e, f)))
            for a, b, e, f in zip(one, q1, q2, q3)
        )

    own = (fin[0], fin[1])
    total = complex_mul(pick(3 - x), own)
    inside = (jnp.zeros_like(dense_r), jnp.zeros_like(dense_r))
    for d in (1, 2, 3):
        theirs = (xbuf[d - 1, 0], xbuf[d - 1, 1])
        total = complex_fma(pick(3 - (x - d + 4) % 4), theirs, total)
        grown = complex_fma((one, q1, q2)[d - 1], theirs, inside)
        inside = tuple(jnp.where(d <= x, a, b) for a, b in zip(grown, inside))
    line[0] = total[0]
    line[1] = total[1]

    def to_line(target, carry):
        remote(line, ybuf.at[ln], ys.at[target], yr.at[ln], (target * 4 + x, k)).start()
        return carry

    lax.fori_loop(ln + 1, 16, to_line, 0)

    meta_copy.wait()
    slot = iota((64, 128), 0)
    chip = (
        ((z + slot // 16) % 4) * 16 + ((y + (slot // 4) % 4) % 4) * 4 + (x + slot % 4) % 4
    )
    expert = (chip * 2 + k).astype(F32)
    before = (iota((128, 128), 0) < iota((128, 128), 1)).astype(F32).astype(BF16)
    sub = iota((64, 8, 128), 1)
    own_meta, other_meta = meta_ref[0:8, :], meta2[...]
    for b in range(2):
        m = jnp.where(k == b, own_meta, other_meta)
        first = m[0:1, :] == expert
        second = m[1:2, :] == expert
        named = jnp.logical_or(first, second)
        rank = dot(named.astype(F32).astype(BF16), before)
        rank = jnp.where(named, rank + 4.0 * b, -1.0)
        weight = jnp.where(first, m[2:3, :], m[3:4, :])
        hit = rank[:, None, :] == sub.astype(F32)
        hot[:, 128 * b : 128 * b + 128] = hit.astype(F32).reshape(512, 128).astype(BF16)
        scaled = jnp.where(hit, weight[:, None, :], 0.0).reshape(512, 128)
        scaled = scaled.T
        high = scaled.astype(BF16)
        comb[b, :, 0:512] = high
        comb[b, :, 512:1024] = (scaled - high.astype(F32)).astype(BF16)

    def from_line(n, acc):
        remote(line, ybuf.at[n], ys.at[0], yr.at[n], (c, other)).wait_recv()
        return complex_fma(q4, acc, (ybuf[n, 0], ybuf[n, 1]))

    earlier = lax.fori_loop(0, ln, from_line, (jnp.zeros_like(dense_r), jnp.zeros_like(dense_r)))
    incoming = complex_fma(pick(x), earlier, inside)

    for j in range(4):
        at = 512 * j
        d1, d32, d64, d128 = segment_powers(j)
        to_seg = (jnp.ones((8, 512), F32), jnp.zeros((8, 512), F32))
        for bit, p in ((1, d32), (2, d64), (4, d128)):
            grown = complex_mul(to_seg, p)
            to_seg = tuple(jnp.where(seg // bit % 2 == 1, a, b) for a, b in zip(grown, to_seg))
        entering = tuple(
            jnp.broadcast_to(lanes_of(v[4 * j : 4 * j + 4, :]), (8, 512)) for v in incoming
        )
        h = complex_fma(to_seg, entering, (edge[0, :, at : at + 512], edge[1, :, at : at + 512]))
        half, base = j // 2, 512 * (j % 2)

        def double_step(i, h):
            rows = pl.ds(pl.multiple_of(i * 16, 16), 16)
            pr, pi = push[0, rows, at : at + 512], push[1, rows, at : at + 512]
            h = complex_fma(d1, h, (pr[0:8], pi[0:8]))
            g = complex_fma(d1, h, (pr[8:16], pi[8:16]))
            st[half, rows, base : base + 512] = jnp.concatenate([h[0], g[0]], axis=0).astype(BF16)
            st[half, rows, 1024 + base : 1536 + base] = jnp.concatenate(
                [h[1], g[1]], axis=0
            ).astype(BF16)
            return g

        lax.fori_loop(0, STEPS // 2, double_step, h, unroll=2)

    read = jnp.concatenate([dot(st[0], cblk[0]), dot(st[1], cblk[1])], axis=1)
    activated = jax.nn.gelu(read + skip_ref[...] * ordered.astype(F32)).astype(BF16)
    pre[k] = dot(unorder, activated).astype(BF16)
    pre_copy = remote(pre.at[k], pre.at[k], psend.at[2], precv.at[2], (c, other))
    pre_copy.start()

    loads[0].wait()
    lin = dot(pre[k], glu[pl.ds(pl.multiple_of(k * 512, 512), 512), :])
    pre_copy.wait()
    lin = lin + dot(pre[other], glu[pl.ds(pl.multiple_of(other * 512, 512), 512), :])
    full = jnp.concatenate([pre[0], pre[1]], axis=1).astype(F32)
    gated = (full * jax.nn.sigmoid(lin)).astype(BF16)
    loads[1].wait()
    loads[2].wait()
    res_copy.wait()
    squares = jnp.zeros((256, 1), F32)
    for n in range(4):
        cols = slice(512 * n, 512 * n + 512)
        start = jnp.concatenate([res[0, :, cols], res[1, :, cols]], axis=0).astype(F32)
        value = start + dot(gated, outw[:, cols])
        squares = squares + jnp.sum(value * value, axis=1, keepdims=True)
        mixed[:, cols] = value
    scale = lax.rsqrt(squares * (1.0 / 2048.0) + EPSILON)
    for n in range(4):
        cols = slice(512 * n, 512 * n + 512)
        normed[:, cols] = (mixed[:, cols] * scale * gain_ref[:, cols]).astype(BF16)
    for n in range(4):
        cols = slice(512 * n, 512 * n + 512)
        send[:, :, cols] = dot(hot[...], normed[:, cols]).reshape(64, 8, 512).astype(BF16)

    def dispatch(i, carry):
        q = i // PER_CHUNK
        remote(send.at[i], recv.at[i], ssem.at[q], rsem.at[q], (chip_at(i, 1), k)).start()
        return carry

    lax.fori_loop(1, 64, dispatch, 0)
    recv[0] = send[0]
    for n in (3, 4, 5):
        loads[n].wait()

    def arrived(buffer, sem, q, first):
        rows = pl.ds(q * PER_CHUNK + first, PER_CHUNK - first)
        return remote(buffer.at[rows], buffer.at[rows], sem.at[q], sem.at[q], (c, other))

    for q in range(CHUNKS):
        first = 1 if q == 0 else 0
        arrived(recv, rsem, q, first).wait_recv()
        rows_in = recv[PER_CHUNK * q : PER_CHUNK * q + PER_CHUNK].reshape(128, 2048)
        gate_part = dot(rows_in, wg[...])
        up_part = dot(rows_in, wu[...])
        hidden = (gate_part * jax.nn.sigmoid(gate_part) * up_part).astype(BF16)
        answer = dot(hidden, wd[...]).astype(BF16)
        ans[PER_CHUNK * q : PER_CHUNK * q + PER_CHUNK] = answer.reshape(PER_CHUNK, 8, 2048)

        def give_back(i, carry):
            remote(ans.at[i], ret.at[i], asem.at[q], bsem.at[q], (chip_at(i, -1), k)).start()
            return carry

        lax.fori_loop(PER_CHUNK * q + first, PER_CHUNK * q + PER_CHUNK, give_back, 0)
        if q == 0:
            ret[0] = ans[0]

    for q in range(CHUNKS):
        first = 1 if q == 0 else 0
        arrived(ret, bsem, q, first).wait_recv()
    returned = ret[...].reshape(512, 2048)
    theirs = comb[other]
    mine = comb[k]
    part_out[...] = (dot(theirs[:, 0:512], returned) + dot(theirs[:, 512:1024], returned)).astype(BF16)
    part_copy = remote(part_out, part_in, psend.at[3], precv.at[3], (c, other))
    part_copy.start()
    routed = dot(mine[:, 0:512], returned) + dot(mine[:, 512:1024], returned)
    routed = routed + mixed[pl.ds(pl.multiple_of(k * 128, 128), 128), :]
    part_copy.wait()
    o_ref[...] = (routed + part_in[...].astype(F32)).astype(BF16)

    def line_sent(target, carry):
        remote(line, ybuf.at[ln], ys.at[target], yr.at[ln], (target * 4 + x, k)).wait_send()
        return carry

    lax.fori_loop(ln + 1, 16, line_sent, 0)
    for q in range(CHUNKS):
        first = 1 if q == 0 else 0
        arrived(send, ssem, q, first).wait_send()
        arrived(ans, asem, q, first).wait_send()


def on_device(
    ssm_input, lam_real, lam_imag, state_in, read_out, channel_skip, glu_weight, out_weight,
    residual, norm_gain, expert_ids, route_weight, expert_gate, expert_up, expert_down,
):
    meta = jnp.concatenate(
        [
            expert_ids.T.astype(F32),
            route_weight.T,
            jnp.zeros((4, 128), F32),
            lam_real.reshape(16, 128),
            lam_imag.reshape(16, 128),
        ]
    )
    vmem = pl.BlockSpec(memory_space=pltpu.VMEM)
    hbm = pl.BlockSpec(memory_space=pl.ANY)
    dma = pltpu.SemaphoreType.DMA
    return pl.pallas_call(
        body,
        out_shape=jax.ShapeDtypeStruct((128, 2048), BF16),
        in_specs=[vmem] * 8 + [hbm] * 6,
        out_specs=vmem,
        scratch_shapes=[
            pltpu.VMEM((1024, 1024), BF16),
            pltpu.VMEM((1024, 2048), BF16),
            pltpu.VMEM((2, 128, 2048), BF16),
            pltpu.VMEM((2048, 512), BF16),
            pltpu.VMEM((2048, 512), BF16),
            pltpu.VMEM((512, 2048), BF16),
            pltpu.VMEM((8, 128), F32),
            pltpu.VMEM((2, 256, 2048), F32),
            pltpu.VMEM((2, 8, 2048), F32),
            pltpu.VMEM((2, 16, 128), F32),
            pltpu.VMEM((3, 2, 16, 128), F32),
            pltpu.VMEM((16, 2, 16, 128), F32),
            pltpu.VMEM((2, 16, 128), F32),
            pltpu.VMEM((2, 256, 2048), BF16),
            pltpu.VMEM((2, 2048, 256), BF16),
            pltpu.VMEM((512, 256), BF16),
            pltpu.VMEM((2, 128, 1024), BF16),
            pltpu.VMEM((2, 256, 512), BF16),
            pltpu.VMEM((256, 2048), F32),
            pltpu.VMEM((256, 2048), BF16),
            pltpu.VMEM((64, 8, 2048), BF16),
            pltpu.VMEM((64, 8, 2048), BF16),
            pltpu.VMEM((64, 8, 2048), BF16),
            pltpu.VMEM((64, 8, 2048), BF16),
            pltpu.VMEM((128, 2048), BF16),
            pltpu.VMEM((128, 2048), BF16),
            dma((6,)), dma((3,)), dma((3,)), dma((16,)), dma((16,)), dma((4,)), dma((4,)),
            dma((4,)), dma((4,)), dma((4,)), dma((4,)),
        ],
        compiler_params=pltpu.CompilerParams(
            collective_id=0, has_side_effects=True, vmem_limit_bytes=60 * 1024 * 1024
        ),
    )(
        ssm_input, lam_real, lam_imag, state_in.reshape(2, 512, 64), read_out,
        channel_skip.reshape(1, 512), norm_gain.reshape(1, 2048), meta,
        glu_weight, out_weight, residual, expert_gate, expert_up, expert_down,
    )


def solution(mesh):
    both = P(("sp", "tp"), None)
    each = P(("sp", "tp"), None, None)
    in_specs = (
        P("sp", "tp"), P("tp", None), P("tp", None), P(None, "tp", None, None), P("tp", None, None),
        P("tp"), P(), P(), both, P(), both, both, each, each, each,
    )
    return jax.shard_map(on_device, mesh=mesh, in_specs=in_specs, out_specs=both, check_vma=False)
```

```python
import functools

import jax
import jax.numpy as jnp
from jax import lax
from jax.experimental import pallas as pl
from jax.experimental.pallas import tpu as pltpu
from jax.sharding import PartitionSpec as P

EPSILON = 1e-06
F32 = jnp.float32
BF16 = jnp.bfloat16
MESH = pl.DeviceIdType.MESH
SEG = 8
STEPS = 32
CHUNKS = 4
PER_CHUNK = 16


def dot(a, b):
    return jnp.dot(a, b, preferred_element_type=F32)


def dot_t(a, b):
    return lax.dot_general(a, b, (((1,), (1,)), ((), ())), preferred_element_type=F32)


def iota(shape, dim):
    return lax.broadcasted_iota(jnp.int32, shape, dim)


def complex_mul(a, b):
    return a[0] * b[0] - a[1] * b[1], a[0] * b[1] + a[1] * b[0]


def complex_fma(a, b, c):
    return a[0] * b[0] - a[1] * b[1] + c[0], a[0] * b[1] + a[1] * b[0] + c[1]


def power(lam_real, lam_imag, exponent):
    magnitude = jnp.exp(exponent * lam_real)
    angle = exponent * lam_imag
    turns = jnp.floor(angle * 0.15915494309189535 + 0.5)
    angle = (angle - turns * 6.28125) - turns * 0.0019353071795864769
    return magnitude * jnp.cos(angle), magnitude * jnp.sin(angle)


def lanes_of(rows):
    return jnp.concatenate([rows[i : i + 1, :] for i in range(rows.shape[0])], axis=1)


def body(
    u_ref, lr_ref, li_ref, in_ref, ro_ref, skip_ref, gain_ref, ids_ref, rw_ref,
    glu_hbm, outw_hbm, res_hbm, wg_hbm, wu_hbm, wd_hbm,
    o_ref,
    glu, outw, res, wg, wu, wd, ids2, rw2,
    push, edge, fin, xbuf, ybuf, line, st, cblk, hot, comb,
    pre, mixed, normed, send, recv, ans, ret, part_out, part_in,
    hsem, xs, xr, ys, yr, psend, precv, ssem, rsem, asem, bsem,
):
    c = lax.axis_index("sp")
    k = lax.axis_index("tp")
    other = 1 - k
    z, y, x = c // 16, (c // 4) % 4, c % 4
    ln = c // 4

    def chip_at(i, sign):
        dz, dy, dx = i // 16, (i // 4) % 4, i % 4
        return (
            ((z + sign * dz + 4) % 4) * 16 + ((y + sign * dy + 4) % 4) * 4 + (x + sign * dx + 4) % 4
        )

    loads = [
        pltpu.make_async_copy(glu_hbm, glu, hsem.at[0]),
        pltpu.make_async_copy(outw_hbm, outw, hsem.at[1]),
        pltpu.make_async_copy(res_hbm, res.at[k], hsem.at[2]),
        pltpu.make_async_copy(wg_hbm.at[0], wg, hsem.at[3]),
        pltpu.make_async_copy(wu_hbm.at[0], wu, hsem.at[4]),
        pltpu.make_async_copy(wd_hbm.at[0], wd, hsem.at[5]),
    ]
    for load in loads:
        load.start()

    barrier = pltpu.get_barrier_semaphore()
    pl.semaphore_signal(barrier, inc=1, device_id=(c, other), device_id_type=MESH)

    def greet(i, carry):
        pl.semaphore_signal(barrier, inc=1, device_id=(chip_at(i, 1), k), device_id_type=MESH)
        return carry

    lax.fori_loop(1, 64, greet, 0)

    lam_r, lam_i = lr_ref[...], li_ref[...]
    decay_re, decay_im = power(lam_r, lam_i, 1.0)
    numer_re = decay_re - 1.0
    denom = lam_r * lam_r + lam_i * lam_i
    hold_re = (numer_re * lam_r + decay_im * lam_i) / denom
    hold_im = (decay_im * lam_r - numer_re * lam_i) / denom
    hold_re = jnp.broadcast_to(hold_re[:, None, :], (32, 16, 64)).reshape(512, 64)
    hold_im = jnp.broadcast_to(hold_im[:, None, :], (32, 16, 64)).reshape(512, 64)
    drive = (
        (hold_re * in_ref[0] - hold_im * in_ref[1]).astype(BF16),
        (hold_re * in_ref[1] + hold_im * in_ref[0]).astype(BF16),
    )
    spread = (iota((64, 1024), 1) % 64 == iota((64, 1024), 0)).astype(F32).astype(BF16)
    own_block = iota((256, 1024), 0) // 16 == iota((256, 1024), 1) // 64
    row, col = iota((256, 256), 0), iota((256, 256), 1)
    order = (col == (row % SEG) * STEPS + row // SEG).astype(F32).astype(BF16)
    unorder = (row == (col % SEG) * STEPS + col // SEG).astype(F32).astype(BF16)
    ordered = dot(order, u_ref[...]).astype(BF16)
    for half in range(2):
        for part in range(2):
            block = dot(drive[part][256 * half : 256 * half + 256], spread)
            block = jnp.where(own_block, block, 0.0).astype(BF16)
            push[part, :, 1024 * half : 1024 * half + 1024] = dot(
                ordered[:, 256 * half : 256 * half + 256], block
            )

    def dense(ref):
        return jnp.concatenate([ref[pl.ds(n, 16, stride=2), :] for n in range(2)], axis=1)

    dense_r, dense_i = dense(lr_ref), dense(li_ref)
    p1 = power(dense_r, dense_i, 1.0)
    p32 = power(dense_r, dense_i, 32.0)
    p64 = power(dense_r, dense_i, 64.0)
    p128 = power(dense_r, dense_i, 128.0)
    q1 = power(dense_r, dense_i, 256.0)
    q2 = complex_mul(q1, q1)
    q3 = complex_mul(q2, q1)
    q4 = complex_mul(q2, q2)
    one = (jnp.ones_like(dense_r), jnp.zeros_like(dense_r))

    def segment_powers(j):
        def lane(v):
            return jnp.broadcast_to(lanes_of(v[4 * j : 4 * j + 4, :]), (8, 512))

        return [tuple(lane(v) for v in p) for p in (p1, p32, p64, p128)]

    seg = iota((8, 512), 0)
    for j in range(4):
        at = 512 * j
        d1, d32, d64, d128 = segment_powers(j)

        def step(i, h):
            rows = pl.ds(pl.multiple_of(i * 8, 8), 8)
            return complex_fma(d1, h, (push[0, rows, at : at + 512], push[1, rows, at : at + 512]))

        zero = jnp.zeros((8, 512), F32)
        h = lax.fori_loop(0, STEPS, step, (zero, zero), unroll=4)
        for d, p in ((1, d32), (2, d64), (4, d128)):
            moved = tuple(jnp.where(seg >= d, pltpu.roll(v, d, 0), 0.0) for v in h)
            h = complex_fma(p, moved, h)
        for part in range(2):
            edge[part, :, at : at + 512] = jnp.where(seg >= 1, pltpu.roll(h[part], 1, 0), 0.0)
            for n in range(4):
                fin[part, 4 * j + n : 4 * j + n + 1, :] = h[part][7:8, 128 * n : 128 * n + 128]

    pl.semaphore_wait(barrier, 64)

    def remote(src, dst, s, r, device):
        return pltpu.make_async_remote_copy(
            src_ref=src, dst_ref=dst, send_sem=s, recv_sem=r, device_id=device, device_id_type=MESH
        )

    along = [
        remote(fin, xbuf.at[d - 1], xs.at[d - 1], xr.at[d - 1], (c - x + (x + d) % 4, k))
        for d in (1, 2, 3)
    ]
    for copy in along:
        copy.start()
    ids_copy = remote(ids_ref, ids2, psend.at[0], precv.at[0], (c, other))
    ids_copy.start()
    rw_copy = remote(rw_ref, rw2, psend.at[4], precv.at[4], (c, other))
    rw_copy.start()
    res_copy = remote(res_hbm, res.at[k], psend.at[1], precv.at[1], (c, other))
    res_copy.start()

    for half in range(2):
        for part in range(2):
            piece = ro_ref[16 * half : 16 * half + 16, :, 64 * part : 64 * part + 64]
            piece = dot(piece.reshape(256, 64).astype(BF16), spread)
            cblk[half, :, 1024 * part : 1024 * part + 1024] = jnp.where(own_block, piece, 0.0).astype(BF16)

    for copy in along:
        copy.wait()

    def pick(n):
        return tuple(
            jnp.where(n == 0, a, jnp.where(n == 1, b, jnp.where(n == 2, e, f)))
            for a, b, e, f in zip(one, q1, q2, q3)
        )

    own = (fin[0], fin[1])
    total = complex_mul(pick(3 - x), own)
    inside = (jnp.zeros_like(dense_r), jnp.zeros_like(dense_r))
    for d in (1, 2, 3):
        theirs = (xbuf[d - 1, 0], xbuf[d - 1, 1])
        total = complex_fma(pick(3 - (x - d + 4) % 4), theirs, total)
        grown = complex_fma((one, q1, q2)[d - 1], theirs, inside)
        inside = tuple(jnp.where(d <= x, a, b) for a, b in zip(grown, inside))
    line[0] = total[0]
    line[1] = total[1]

    def to_line(target, carry):
        remote(line, ybuf.at[ln], ys.at[target], yr.at[ln], (target * 4 + x, k)).start()
        return carry

    lax.fori_loop(ln + 1, 16, to_line, 0)

    ids_copy.wait()
    rw_copy.wait()
    slot = iota((64, 128), 0)
    chip = (
        ((z + slot // 16) % 4) * 16 + ((y + (slot // 4) % 4) % 4) * 4 + (x + slot % 4) % 4
    )
    expert = chip * 2 + k
    before = (iota((128, 128), 0) < iota((128, 128), 1)).astype(F32).astype(BF16)
    sub = iota((64, 8, 128), 1)
    for b in range(2):
        ids = jnp.where(k == b, ids_ref[...], ids2[...])
        weights = jnp.where(k == b, rw_ref[...], rw2[...])
        first = ids[0:1, :] == expert
        second = ids[1:2, :] == expert
        named = jnp.logical_or(first, second)
        rank = dot(named.astype(F32).astype(BF16), before)
        rank = jnp.where(named, rank + 4.0 * b, -1.0)
        weight = jnp.where(first, weights[0:1, :], weights[1:2, :])
        hit = rank[:, None, :] == sub.astype(F32)
        hot[:, 128 * b : 128 * b + 128] = hit.astype(F32).reshape(512, 128).astype(BF16)
        scaled = jnp.where(hit, weight[:, None, :], 0.0).reshape(512, 128)
        scaled = scaled.T
        high = scaled.astype(BF16)
        comb[b, :, 0:512] = high
        comb[b, :, 512:1024] = (scaled - high.astype(F32)).astype(BF16)

    def from_line(n, acc):
        remote(line, ybuf.at[n], ys.at[0], yr.at[n], (c, other)).wait_recv()
        return complex_fma(q4, acc, (ybuf[n, 0], ybuf[n, 1]))

    earlier = lax.fori_loop(0, ln, from_line, (jnp.zeros_like(dense_r), jnp.zeros_like(dense_r)))
    incoming = complex_fma(pick(x), earlier, inside)

    for j in range(4):
        at = 512 * j
        d1, d32, d64, d128 = segment_powers(j)
        to_seg = (jnp.ones((8, 512), F32), jnp.zeros((8, 512), F32))
        for bit, p in ((1, d32), (2, d64), (4, d128)):
            grown = complex_mul(to_seg, p)
            to_seg = tuple(jnp.where(seg // bit % 2 == 1, a, b) for a, b in zip(grown, to_seg))
        entering = tuple(
            jnp.broadcast_to(lanes_of(v[4 * j : 4 * j + 4, :]), (8, 512)) for v in incoming
        )
        h = complex_fma(to_seg, entering, (edge[0, :, at : at + 512], edge[1, :, at : at + 512]))
        half, base = j // 2, 512 * (j % 2)

        def double_step(i, h):
            rows = pl.ds(pl.multiple_of(i * 16, 16), 16)
            pr, pi = push[0, rows, at : at + 512], push[1, rows, at : at + 512]
            h = complex_fma(d1, h, (pr[0:8], pi[0:8]))
            g = complex_fma(d1, h, (pr[8:16], pi[8:16]))
            st[half, rows, base : base + 512] = jnp.concatenate([h[0], g[0]], axis=0).astype(BF16)
            st[half, rows, 1024 + base : 1536 + base] = jnp.concatenate(
                [h[1], g[1]], axis=0
            ).astype(BF16)
            return g

        lax.fori_loop(0, STEPS // 2, double_step, h, unroll=2)

    read = jnp.concatenate([dot_t(st[0], cblk[0]), dot_t(st[1], cblk[1])], axis=1)
    activated = jax.nn.gelu(read + skip_ref[...] * ordered.astype(F32)).astype(BF16)
    pre[k] = dot(unorder, activated).astype(BF16)
    pre_copy = remote(pre.at[k], pre.at[k], psend.at[2], precv.at[2], (c, other))
    pre_copy.start()

    loads[0].wait()
    lin = dot(pre[k], glu[pl.ds(pl.multiple_of(k * 512, 512), 512), :])
    pre_copy.wait()
    lin = lin + dot(pre[other], glu[pl.ds(pl.multiple_of(other * 512, 512), 512), :])
    full = jnp.concatenate([pre[0], pre[1]], axis=1).astype(F32)
    gated = (full * jax.nn.sigmoid(lin)).astype(BF16)
    loads[1].wait()
    loads[2].wait()
    res_copy.wait()
    squares = jnp.zeros((256, 1), F32)
    for n in range(4):
        cols = slice(512 * n, 512 * n + 512)
        start = jnp.concatenate([res[0, :, cols], res[1, :, cols]], axis=0).astype(F32)
        value = start + dot(gated, outw[:, cols])
        squares = squares + jnp.sum(value * value, axis=1, keepdims=True)
        mixed[:, cols] = value
    scale = lax.rsqrt(squares * (1.0 / 2048.0) + EPSILON)
    for n in range(4):
        cols = slice(512 * n, 512 * n + 512)
        normed[:, cols] = (mixed[:, cols] * scale * gain_ref[:, cols]).astype(BF16)
    for n in range(4):
        cols = slice(512 * n, 512 * n + 512)
        send[:, :, cols] = dot(hot[...], normed[:, cols]).reshape(64, 8, 512).astype(BF16)

    def dispatch(i, carry):
        q = i // PER_CHUNK
        remote(send.at[i], recv.at[i], ssem.at[q], rsem.at[q], (chip_at(i, 1), k)).start()
        return carry

    lax.fori_loop(1, 64, dispatch, 0)
    recv[0] = send[0]
    for n in (3, 4, 5):
        loads[n].wait()

    def arrived(buffer, sem, q, first):
        rows = pl.ds(q * PER_CHUNK + first, PER_CHUNK - first)
        return remote(buffer.at[rows], buffer.at[rows], sem.at[q], sem.at[q], (c, other))

    for q in range(CHUNKS):
        first = 1 if q == 0 else 0
        arrived(recv, rsem, q, first).wait_recv()
        rows_in = recv[PER_CHUNK * q : PER_CHUNK * q + PER_CHUNK].reshape(128, 2048)
        gate_part = dot(rows_in, wg[...])
        up_part = dot(rows_in, wu[...])
        hidden = (gate_part * jax.nn.sigmoid(gate_part) * up_part).astype(BF16)
        answer = dot(hidden, wd[...]).astype(BF16)
        ans[PER_CHUNK * q : PER_CHUNK * q + PER_CHUNK] = answer.reshape(PER_CHUNK, 8, 2048)

        def give_back(i, carry):
            remote(ans.at[i], ret.at[i], asem.at[q], bsem.at[q], (chip_at(i, -1), k)).start()
            return carry

        lax.fori_loop(PER_CHUNK * q + first, PER_CHUNK * q + PER_CHUNK, give_back, 0)
        if q == 0:
            ret[0] = ans[0]

    for q in range(CHUNKS):
        first = 1 if q == 0 else 0
        arrived(ret, bsem, q, first).wait_recv()
    returned = ret[...].reshape(512, 2048)
    theirs = comb[other]
    mine = comb[k]
    part_out[...] = (dot(theirs[:, 0:512], returned) + dot(theirs[:, 512:1024], returned)).astype(BF16)
    part_copy = remote(part_out, part_in, psend.at[3], precv.at[3], (c, other))
    part_copy.start()
    routed = dot(mine[:, 0:512], returned) + dot(mine[:, 512:1024], returned)
    routed = routed + mixed[pl.ds(pl.multiple_of(k * 128, 128), 128), :]
    part_copy.wait()
    o_ref[...] = (routed + part_in[...].astype(F32)).astype(BF16)

    def line_sent(target, carry):
        remote(line, ybuf.at[ln], ys.at[target], yr.at[ln], (target * 4 + x, k)).wait_send()
        return carry

    lax.fori_loop(ln + 1, 16, line_sent, 0)
    for q in range(CHUNKS):
        first = 1 if q == 0 else 0
        arrived(send, ssem, q, first).wait_send()
        arrived(ans, asem, q, first).wait_send()


def on_device(
    ssm_input, lam_real, lam_imag, state_in, read_out, channel_skip, glu_weight, out_weight,
    residual, norm_gain, expert_ids, route_weight, expert_gate, expert_up, expert_down,
):
    vmem = pl.BlockSpec(memory_space=pltpu.VMEM)
    hbm = pl.BlockSpec(memory_space=pl.ANY)
    dma = pltpu.SemaphoreType.DMA
    return pl.pallas_call(
        body,
        out_shape=jax.ShapeDtypeStruct((128, 2048), BF16),
        in_specs=[vmem] * 9 + [hbm] * 6,
        out_specs=vmem,
        scratch_shapes=[
            pltpu.VMEM((1024, 1024), BF16),
            pltpu.VMEM((1024, 2048), BF16),
            pltpu.VMEM((2, 128, 2048), BF16),
            pltpu.VMEM((2048, 512), BF16),
            pltpu.VMEM((2048, 512), BF16),
            pltpu.VMEM((512, 2048), BF16),
            pltpu.VMEM((2, 128), jnp.int32),
            pltpu.VMEM((2, 128), F32),
            pltpu.VMEM((2, 256, 2048), F32),
            pltpu.VMEM((2, 8, 2048), F32),
            pltpu.VMEM((2, 16, 128), F32),
            pltpu.VMEM((3, 2, 16, 128), F32),
            pltpu.VMEM((16, 2, 16, 128), F32),
            pltpu.VMEM((2, 16, 128), F32),
            pltpu.VMEM((2, 256, 2048), BF16),
            pltpu.VMEM((2, 256, 2048), BF16),
            pltpu.VMEM((512, 256), BF16),
            pltpu.VMEM((2, 128, 1024), BF16),
            pltpu.VMEM((2, 256, 512), BF16),
            pltpu.VMEM((256, 2048), F32),
            pltpu.VMEM((256, 2048), BF16),
            pltpu.VMEM((64, 8, 2048), BF16),
            pltpu.VMEM((64, 8, 2048), BF16),
            pltpu.VMEM((64, 8, 2048), BF16),
            pltpu.VMEM((64, 8, 2048), BF16),
            pltpu.VMEM((128, 2048), BF16),
            pltpu.VMEM((128, 2048), BF16),
            dma((6,)), dma((3,)), dma((3,)), dma((16,)), dma((16,)), dma((5,)), dma((5,)),
            dma((4,)), dma((4,)), dma((4,)), dma((4,)),
        ],
        compiler_params=pltpu.CompilerParams(
            collective_id=0, has_side_effects=True, vmem_limit_bytes=60 * 1024 * 1024
        ),
    )(
        ssm_input, lam_real, lam_imag, state_in.reshape(2, 512, 64),
        read_out.transpose(0, 2, 1), channel_skip.reshape(1, 512), norm_gain.reshape(1, 2048),
        expert_ids.T, route_weight.T,
        glu_weight, out_weight, residual, expert_gate, expert_up, expert_down,
    )


def solution(mesh):
    both = P(("sp", "tp"), None)
    each = P(("sp", "tp"), None, None)
    in_specs = (
        P("sp", "tp"), P("tp", None), P("tp", None), P(None, "tp", None, None), P("tp", None, None),
        P("tp"), P(), P(), both, P(), both, both, each, each, each,
    )
    return jax.shard_map(on_device, mesh=mesh, in_specs=in_specs, out_specs=both, check_vma=False)
```

```python
import functools

import jax
import jax.numpy as jnp
from jax import lax
from jax.experimental import pallas as pl
from jax.experimental.pallas import tpu as pltpu
from jax.sharding import PartitionSpec as P

EPSILON = 1e-06
F32 = jnp.float32
BF16 = jnp.bfloat16
MESH = pl.DeviceIdType.MESH
SEG = 8
STEPS = 32
CHUNKS = 4
PER_CHUNK = 16


def steps_of(shift):
    both = []
    for d in shift:
        both += [float(d == 1) + float(d == 2), float(d == 3) + float(d == 2)]
    return both


def balanced_order():
    left = [(n // 16, n // 4 % 4, n % 4) for n in range(1, 64)]
    total, order = [0.0] * 6, [(0, 0, 0)]
    while left:

        def cost(shift):
            now = [a + b for a, b in zip(total, steps_of(shift))]
            return (max(now) - min(now), -sum(steps_of(shift)))

        best = min(left, key=cost)
        left.remove(best)
        order.append(best)
        total = [a + b for a, b in zip(total, steps_of(best))]
    return order


ORDER = balanced_order()


def dot(a, b):
    return jnp.dot(a, b, preferred_element_type=F32)


def dot_t(a, b):
    return lax.dot_general(a, b, (((1,), (1,)), ((), ())), preferred_element_type=F32)


def iota(shape, dim):
    return lax.broadcasted_iota(jnp.int32, shape, dim)


def complex_mul(a, b):
    return a[0] * b[0] - a[1] * b[1], a[0] * b[1] + a[1] * b[0]


def complex_fma(a, b, c):
    return a[0] * b[0] - a[1] * b[1] + c[0], a[0] * b[1] + a[1] * b[0] + c[1]


def power(lam_real, lam_imag, exponent):
    magnitude = jnp.exp(exponent * lam_real)
    angle = exponent * lam_imag
    turns = jnp.floor(angle * 0.15915494309189535 + 0.5)
    angle = (angle - turns * 6.28125) - turns * 0.0019353071795864769
    return magnitude * jnp.cos(angle), magnitude * jnp.sin(angle)


def lanes_of(rows):
    return jnp.concatenate([rows[i : i + 1, :] for i in range(rows.shape[0])], axis=1)


def body(
    u_ref, lr_ref, li_ref, in_ref, ro_ref, skip_ref, gain_ref, ids_ref, rw_ref,
    glu_hbm, outw_hbm, res_hbm, wg_hbm, wu_hbm, wd_hbm,
    o_ref,
    glu, outw, res, wg, wu, wd, ids2, rw2,
    push, edge, fin, xbuf, ybuf, line, st, cblk, hot, comb,
    pre, mixed, normed, send, recv, ans, ret, part_out, part_in, part_sum, own_sum,
    hsem, xs, xr, ys, yr, psend, precv, ssem, rsem, asem, bsem,
):
    c = lax.axis_index("sp")
    k = lax.axis_index("tp")
    other = 1 - k
    z, y, x = c // 16, (c // 4) % 4, c % 4
    ln = c // 4

    def chip_at(shift, sign):
        dz, dy, dx = (sign * d % 4 for d in shift)
        return ((z + dz) % 4) * 16 + ((y + dy) % 4) * 4 + (x + dx) % 4

    loads = [
        pltpu.make_async_copy(glu_hbm, glu, hsem.at[0]),
        pltpu.make_async_copy(outw_hbm, outw, hsem.at[1]),
        pltpu.make_async_copy(res_hbm, res.at[k], hsem.at[2]),
        pltpu.make_async_copy(wg_hbm.at[0], wg, hsem.at[3]),
        pltpu.make_async_copy(wu_hbm.at[0], wu, hsem.at[4]),
        pltpu.make_async_copy(wd_hbm.at[0], wd, hsem.at[5]),
    ]
    for load in loads:
        load.start()

    barrier = pltpu.get_barrier_semaphore()
    pl.semaphore_signal(barrier, inc=1, device_id=(c, other), device_id_type=MESH)

    for d in (1, 2, 3):
        pl.semaphore_signal(barrier, inc=1, device_id=(c - x + (x + d) % 4, k), device_id_type=MESH)
    for d in range(1, 16):
        pl.semaphore_signal(barrier, inc=1, device_id=((c + 4 * d) % 64, k), device_id_type=MESH)

    lam_r, lam_i = lr_ref[...], li_ref[...]
    decay_re, decay_im = power(lam_r, lam_i, 1.0)
    numer_re = decay_re - 1.0
    denom = lam_r * lam_r + lam_i * lam_i
    hold_re = (numer_re * lam_r + decay_im * lam_i) / denom
    hold_im = (decay_im * lam_r - numer_re * lam_i) / denom
    hold_re = jnp.broadcast_to(hold_re[:, None, :], (32, 16, 64)).reshape(512, 64)
    hold_im = jnp.broadcast_to(hold_im[:, None, :], (32, 16, 64)).reshape(512, 64)
    drive = (
        (hold_re * in_ref[0] - hold_im * in_ref[1]).astype(BF16),
        (hold_re * in_ref[1] + hold_im * in_ref[0]).astype(BF16),
    )
    spread = (iota((64, 1024), 1) % 64 == iota((64, 1024), 0)).astype(F32).astype(BF16)
    own_block = iota((256, 1024), 0) // 16 == iota((256, 1024), 1) // 64
    row, col = iota((256, 256), 0), iota((256, 256), 1)
    order = (col == (row % SEG) * STEPS + row // SEG).astype(F32).astype(BF16)
    unorder = (row == (col % SEG) * STEPS + col // SEG).astype(F32).astype(BF16)
    ordered = dot(order, u_ref[...]).astype(BF16)
    for half in range(2):
        for part in range(2):
            block = dot(drive[part][256 * half : 256 * half + 256], spread)
            block = jnp.where(own_block, block, 0.0).astype(BF16)
            push[part, :, 1024 * half : 1024 * half + 1024] = dot(
                ordered[:, 256 * half : 256 * half + 256], block
            )

    def dense(ref):
        return jnp.concatenate([ref[pl.ds(n, 16, stride=2), :] for n in range(2)], axis=1)

    dense_r, dense_i = dense(lr_ref), dense(li_ref)
    p1 = power(dense_r, dense_i, 1.0)
    p32 = power(dense_r, dense_i, 32.0)
    p64 = power(dense_r, dense_i, 64.0)
    p128 = power(dense_r, dense_i, 128.0)
    q1 = power(dense_r, dense_i, 256.0)
    q2 = complex_mul(q1, q1)
    q3 = complex_mul(q2, q1)
    q4 = complex_mul(q2, q2)
    one = (jnp.ones_like(dense_r), jnp.zeros_like(dense_r))

    def segment_powers(j):
        def lane(v):
            return jnp.broadcast_to(lanes_of(v[4 * j : 4 * j + 4, :]), (8, 512))

        return [tuple(lane(v) for v in p) for p in (p1, p32, p64, p128)]

    seg = iota((8, 512), 0)
    for j in range(4):
        at = 512 * j
        d1, d32, d64, d128 = segment_powers(j)

        def step(i, h):
            rows = pl.ds(pl.multiple_of(i * 8, 8), 8)
            return complex_fma(d1, h, (push[0, rows, at : at + 512], push[1, rows, at : at + 512]))

        zero = jnp.zeros((8, 512), F32)
        h = lax.fori_loop(0, STEPS, step, (zero, zero), unroll=4)
        for d, p in ((1, d32), (2, d64), (4, d128)):
            moved = tuple(jnp.where(seg >= d, pltpu.roll(v, d, 0), 0.0) for v in h)
            h = complex_fma(p, moved, h)
        for part in range(2):
            edge[part, :, at : at + 512] = jnp.where(seg >= 1, pltpu.roll(h[part], 1, 0), 0.0)
            for n in range(4):
                fin[part, 4 * j + n : 4 * j + n + 1, :] = h[part][7:8, 128 * n : 128 * n + 128]

    pl.semaphore_wait(barrier, 19)

    def remote(src, dst, s, r, device):
        return pltpu.make_async_remote_copy(
            src_ref=src, dst_ref=dst, send_sem=s, recv_sem=r, device_id=device, device_id_type=MESH
        )

    along = [
        remote(fin, xbuf.at[d - 1], xs.at[d - 1], xr.at[d - 1], (c - x + (x + d) % 4, k))
        for d in (1, 2, 3)
    ]
    for copy in along:
        copy.start()
    ids_copy = remote(ids_ref, ids2, psend.at[0], precv.at[0], (c, other))
    ids_copy.start()
    rw_copy = remote(rw_ref, rw2, psend.at[4], precv.at[4], (c, other))
    rw_copy.start()
    res_copy = remote(res_hbm, res.at[k], psend.at[1], precv.at[1], (c, other))
    res_copy.start()

    for half in range(2):
        for part in range(2):
            piece = ro_ref[16 * half : 16 * half + 16, :, 64 * part : 64 * part + 64]
            piece = dot(piece.reshape(256, 64).astype(BF16), spread)
            cblk[half, :, 1024 * part : 1024 * part + 1024] = jnp.where(own_block, piece, 0.0).astype(BF16)

    for copy in along:
        copy.wait()

    def pick(n):
        return tuple(
            jnp.where(n == 0, a, jnp.where(n == 1, b, jnp.where(n == 2, e, f)))
            for a, b, e, f in zip(one, q1, q2, q3)
        )

    own = (fin[0], fin[1])
    total = complex_mul(pick(3 - x), own)
    inside = (jnp.zeros_like(dense_r), jnp.zeros_like(dense_r))
    for d in (1, 2, 3):
        theirs = (xbuf[d - 1, 0], xbuf[d - 1, 1])
        total = complex_fma(pick(3 - (x - d + 4) % 4), theirs, total)
        grown = complex_fma((one, q1, q2)[d - 1], theirs, inside)
        inside = tuple(jnp.where(d <= x, a, b) for a, b in zip(grown, inside))
    line[0] = total[0]
    line[1] = total[1]

    def to_line(target, carry):
        remote(line, ybuf.at[ln], ys.at[target], yr.at[ln], (target * 4 + x, k)).start()
        return carry

    lax.fori_loop(ln + 1, 16, to_line, 0)

    ids_copy.wait()
    rw_copy.wait()
    slot = iota((64, 128), 0)
    code = jnp.zeros((64, 128), jnp.int32)
    for n, (dz, dy, dx) in enumerate(ORDER):
        code = jnp.where(slot == n, dz * 16 + dy * 4 + dx, code)
    chip = ((z + code // 16) % 4) * 16 + ((y + code // 4 % 4) % 4) * 4 + (x + code % 4) % 4
    expert = chip * 2 + k
    before = (iota((128, 128), 0) < iota((128, 128), 1)).astype(F32).astype(BF16)
    sub = iota((64, 8, 128), 1)
    for b in range(2):
        ids = jnp.where(k == b, ids_ref[...], ids2[...])
        weights = jnp.where(k == b, rw_ref[...], rw2[...])
        first = ids[0:1, :] == expert
        second = ids[1:2, :] == expert
        named = jnp.logical_or(first, second)
        rank = dot(named.astype(F32).astype(BF16), before)
        rank = jnp.where(named, rank + 4.0 * b, -1.0)
        weight = jnp.where(first, weights[0:1, :], weights[1:2, :])
        hit = rank[:, None, :] == sub.astype(F32)
        hot[:, 128 * b : 128 * b + 128] = hit.astype(F32).reshape(512, 128).astype(BF16)
        scaled = jnp.where(hit, weight[:, None, :], 0.0).reshape(512, 128)
        scaled = scaled.T
        high = scaled.astype(BF16)
        comb[b, :, 0:512] = high
        comb[b, :, 512:1024] = (scaled - high.astype(F32)).astype(BF16)

    def from_line(n, acc):
        remote(line, ybuf.at[n], ys.at[0], yr.at[n], (c, other)).wait_recv()
        return complex_fma(q4, acc, (ybuf[n, 0], ybuf[n, 1]))

    earlier = lax.fori_loop(0, ln, from_line, (jnp.zeros_like(dense_r), jnp.zeros_like(dense_r)))
    incoming = complex_fma(pick(x), earlier, inside)

    for j in range(4):
        at = 512 * j
        d1, d32, d64, d128 = segment_powers(j)
        to_seg = (jnp.ones((8, 512), F32), jnp.zeros((8, 512), F32))
        for bit, p in ((1, d32), (2, d64), (4, d128)):
            grown = complex_mul(to_seg, p)
            to_seg = tuple(jnp.where(seg // bit % 2 == 1, a, b) for a, b in zip(grown, to_seg))
        entering = tuple(
            jnp.broadcast_to(lanes_of(v[4 * j : 4 * j + 4, :]), (8, 512)) for v in incoming
        )
        h = complex_fma(to_seg, entering, (edge[0, :, at : at + 512], edge[1, :, at : at + 512]))
        half, base = j // 2, 512 * (j % 2)

        def double_step(i, h):
            rows = pl.ds(pl.multiple_of(i * 16, 16), 16)
            pr, pi = push[0, rows, at : at + 512], push[1, rows, at : at + 512]
            h = complex_fma(d1, h, (pr[0:8], pi[0:8]))
            g = complex_fma(d1, h, (pr[8:16], pi[8:16]))
            st[half, rows, base : base + 512] = jnp.concatenate([h[0], g[0]], axis=0).astype(BF16)
            st[half, rows, 1024 + base : 1536 + base] = jnp.concatenate(
                [h[1], g[1]], axis=0
            ).astype(BF16)
            return g

        lax.fori_loop(0, STEPS // 2, double_step, h, unroll=2)

    read = jnp.concatenate([dot_t(st[0], cblk[0]), dot_t(st[1], cblk[1])], axis=1)
    activated = jax.nn.gelu(read + skip_ref[...] * ordered.astype(F32)).astype(BF16)
    pre[k] = dot(unorder, activated).astype(BF16)
    pre_copy = remote(pre.at[k], pre.at[k], psend.at[2], precv.at[2], (c, other))
    pre_copy.start()

    loads[0].wait()
    lin = dot(pre[k], glu[pl.ds(pl.multiple_of(k * 512, 512), 512), :])
    pre_copy.wait()
    lin = lin + dot(pre[other], glu[pl.ds(pl.multiple_of(other * 512, 512), 512), :])
    full = jnp.concatenate([pre[0], pre[1]], axis=1).astype(F32)
    gated = (full * jax.nn.sigmoid(lin)).astype(BF16)
    loads[1].wait()
    loads[2].wait()
    res_copy.wait()
    squares = jnp.zeros((256, 1), F32)
    for n in range(4):
        cols = slice(512 * n, 512 * n + 512)
        start = jnp.concatenate([res[0, :, cols], res[1, :, cols]], axis=0).astype(F32)
        value = start + dot(gated, outw[:, cols])
        squares = squares + jnp.sum(value * value, axis=1, keepdims=True)
        mixed[:, cols] = value
    scale = lax.rsqrt(squares * (1.0 / 2048.0) + EPSILON)
    for n in range(4):
        cols = slice(512 * n, 512 * n + 512)
        normed[:, cols] = (mixed[:, cols] * scale * gain_ref[:, cols]).astype(BF16)
    for n in range(4):
        cols = slice(512 * n, 512 * n + 512)
        send[:, :, cols] = dot(hot[...], normed[:, cols]).reshape(64, 8, 512).astype(BF16)

    for n in range(1, 64):
        q = n // PER_CHUNK
        remote(send.at[n], recv.at[n], ssem.at[q], rsem.at[q], (chip_at(ORDER[n], 1), k)).start()
    recv[0] = send[0]
    for n in (3, 4, 5):
        loads[n].wait()

    def arrived(buffer, sem, q):
        first = 1 if q == 0 else 0
        rows = pl.ds(q * PER_CHUNK + first, PER_CHUNK - first)
        return remote(buffer.at[rows], buffer.at[rows], sem.at[q], sem.at[q], (c, other))

    for q in range(CHUNKS):
        arrived(recv, rsem, q).wait_recv()
        slots = slice(PER_CHUNK * q, PER_CHUNK * q + PER_CHUNK)
        rows_in = recv[slots].reshape(8 * PER_CHUNK, 2048)
        gate_part = dot(rows_in, wg[...])
        up_part = dot(rows_in, wu[...])
        hidden = (gate_part * jax.nn.sigmoid(gate_part) * up_part).astype(BF16)
        ans[slots] = dot(hidden, wd[...]).astype(BF16).reshape(PER_CHUNK, 8, 2048)
        for n in range(max(1, PER_CHUNK * q), PER_CHUNK * q + PER_CHUNK):
            remote(ans.at[n], ret.at[n], asem.at[q], bsem.at[q], (chip_at(ORDER[n], -1), k)).start()
        if q == 0:
            ret[0] = ans[0]

    for half in range(2):
        for q in range(half * CHUNKS // 2, (half + 1) * CHUNKS // 2):
            arrived(ret, bsem, q).wait_recv()
        returned = ret[32 * half : 32 * half + 32].reshape(256, 2048)
        high = slice(256 * half, 256 * half + 256)
        low = slice(512 + 256 * half, 768 + 256 * half)
        theirs, mine = comb[other], comb[k]
        routed = dot(theirs[:, high], returned) + dot(theirs[:, low], returned)
        if half == 0:
            part_sum[...] = routed
            own_rows = pl.ds(pl.multiple_of(k * 128, 128), 128)
            own_sum[...] = (
                mixed[own_rows, :] + dot(mine[:, high], returned) + dot(mine[:, low], returned)
            )
        else:
            part_out[...] = (part_sum[...] + routed).astype(BF16)
            part_copy = remote(part_out, part_in, psend.at[3], precv.at[3], (c, other))
            part_copy.start()
            own_sum[...] = own_sum[...] + dot(mine[:, high], returned) + dot(mine[:, low], returned)
    part_copy.wait()
    o_ref[...] = (own_sum[...] + part_in[...].astype(F32)).astype(BF16)

    def line_sent(target, carry):
        remote(line, ybuf.at[ln], ys.at[target], yr.at[ln], (target * 4 + x, k)).wait_send()
        return carry

    lax.fori_loop(ln + 1, 16, line_sent, 0)
    for q in range(CHUNKS):
        arrived(send, ssem, q).wait_send()
        arrived(ans, asem, q).wait_send()


def on_device(
    ssm_input, lam_real, lam_imag, state_in, read_out, channel_skip, glu_weight, out_weight,
    residual, norm_gain, expert_ids, route_weight, expert_gate, expert_up, expert_down,
):
    vmem = pl.BlockSpec(memory_space=pltpu.VMEM)
    hbm = pl.BlockSpec(memory_space=pl.ANY)
    dma = pltpu.SemaphoreType.DMA
    return pl.pallas_call(
        body,
        out_shape=jax.ShapeDtypeStruct((128, 2048), BF16),
        in_specs=[vmem] * 9 + [hbm] * 6,
        out_specs=vmem,
        scratch_shapes=[
            pltpu.VMEM((1024, 1024), BF16),
            pltpu.VMEM((1024, 2048), BF16),
            pltpu.VMEM((2, 128, 2048), BF16),
            pltpu.VMEM((2048, 512), BF16),
            pltpu.VMEM((2048, 512), BF16),
            pltpu.VMEM((512, 2048), BF16),
            pltpu.VMEM((2, 128), jnp.int32),
            pltpu.VMEM((2, 128), F32),
            pltpu.VMEM((2, 256, 2048), F32),
            pltpu.VMEM((2, 8, 2048), F32),
            pltpu.VMEM((2, 16, 128), F32),
            pltpu.VMEM((3, 2, 16, 128), F32),
            pltpu.VMEM((16, 2, 16, 128), F32),
            pltpu.VMEM((2, 16, 128), F32),
            pltpu.VMEM((2, 256, 2048), BF16),
            pltpu.VMEM((2, 256, 2048), BF16),
            pltpu.VMEM((512, 256), BF16),
            pltpu.VMEM((2, 128, 1024), BF16),
            pltpu.VMEM((2, 256, 512), BF16),
            pltpu.VMEM((256, 2048), F32),
            pltpu.VMEM((256, 2048), BF16),
            pltpu.VMEM((64, 8, 2048), BF16),
            pltpu.VMEM((64, 8, 2048), BF16),
            pltpu.VMEM((64, 8, 2048), BF16),
            pltpu.VMEM((64, 8, 2048), BF16),
            pltpu.VMEM((128, 2048), BF16),
            pltpu.VMEM((128, 2048), BF16),
            pltpu.VMEM((128, 2048), F32),
            pltpu.VMEM((128, 2048), F32),
            dma((6,)), dma((3,)), dma((3,)), dma((16,)), dma((16,)), dma((5,)), dma((5,)),
            dma((4,)), dma((4,)), dma((4,)), dma((4,)),
        ],
        compiler_params=pltpu.CompilerParams(
            collective_id=0, has_side_effects=True, vmem_limit_bytes=60 * 1024 * 1024
        ),
    )(
        ssm_input, lam_real, lam_imag, state_in.reshape(2, 512, 64),
        read_out.transpose(0, 2, 1), channel_skip.reshape(1, 512), norm_gain.reshape(1, 2048),
        expert_ids.T, route_weight.T,
        glu_weight, out_weight, residual, expert_gate, expert_up, expert_down,
    )


def solution(mesh):
    both = P(("sp", "tp"), None)
    each = P(("sp", "tp"), None, None)
    in_specs = (
        P("sp", "tp"), P("tp", None), P("tp", None), P(None, "tp", None, None), P("tp", None, None),
        P("tp"), P(), P(), both, P(), both, both, each, each, each,
    )
    return jax.shard_map(on_device, mesh=mesh, in_specs=in_specs, out_specs=both, check_vma=False)
```

```python
import functools

import jax
import jax.numpy as jnp
from jax import lax
from jax.experimental import pallas as pl
from jax.experimental.pallas import tpu as pltpu
from jax.sharding import PartitionSpec as P

EPSILON = 1e-06
F32 = jnp.float32
BF16 = jnp.bfloat16
MESH = pl.DeviceIdType.MESH
SEG = 8
STEPS = 32
CHUNKS = 4
PER_CHUNK = 16
EARLY = 1
EARLY_SLOTS = EARLY * PER_CHUNK


def steps_of(shift):
    both = []
    for d in shift:
        both += [float(d == 1) + float(d == 2), float(d == 3) + float(d == 2)]
    return both


def balanced_order():
    left = [(n // 16, n // 4 % 4, n % 4) for n in range(1, 64)]
    total, order = [0.0] * 6, [(0, 0, 0)]
    while left:

        def cost(shift):
            now = [a + b for a, b in zip(total, steps_of(shift))]
            return (max(now) - min(now), -sum(steps_of(shift)))

        best = min(left, key=cost)
        left.remove(best)
        order.append(best)
        total = [a + b for a, b in zip(total, steps_of(best))]
    return order


ORDER = balanced_order()


def dot(a, b):
    return jnp.dot(a, b, preferred_element_type=F32)


def dot_t(a, b):
    return lax.dot_general(a, b, (((1,), (1,)), ((), ())), preferred_element_type=F32)


def iota(shape, dim):
    return lax.broadcasted_iota(jnp.int32, shape, dim)


def complex_mul(a, b):
    return a[0] * b[0] - a[1] * b[1], a[0] * b[1] + a[1] * b[0]


def complex_fma(a, b, c):
    return a[0] * b[0] - a[1] * b[1] + c[0], a[0] * b[1] + a[1] * b[0] + c[1]


def power(lam_real, lam_imag, exponent):
    magnitude = jnp.exp(exponent * lam_real)
    angle = exponent * lam_imag
    turns = jnp.floor(angle * 0.15915494309189535 + 0.5)
    angle = (angle - turns * 6.28125) - turns * 0.0019353071795864769
    return magnitude * jnp.cos(angle), magnitude * jnp.sin(angle)


def lanes_of(rows):
    return jnp.concatenate([rows[i : i + 1, :] for i in range(rows.shape[0])], axis=1)


def body(
    u_ref, lr_ref, li_ref, in_ref, ro_ref, skip_ref, gain_ref, ids_ref, rw_ref,
    glu_hbm, outw_hbm, res_hbm, wg_hbm, wu_hbm, wd_hbm,
    o_ref,
    glu, outw, res, wg, wu, wd, ids2, rw2,
    push, edge, fin, xbuf, ybuf, line, st, cblk, hot, comb,
    pre, mixed, normed, send, recv, ans, ret, part_out, part_in, part_sum, own_sum, gsend, grecv,
    hsem, xs, xr, ys, yr, psend, precv, ssem, rsem, asem, bsem, gsem, grsem,
):
    c = lax.axis_index("sp")
    k = lax.axis_index("tp")
    other = 1 - k
    z, y, x = c // 16, (c // 4) % 4, c % 4
    ln = c // 4

    def chip_at(shift, sign):
        dz, dy, dx = (sign * d % 4 for d in shift)
        return ((z + dz) % 4) * 16 + ((y + dy) % 4) * 4 + (x + dx) % 4

    loads = [
        pltpu.make_async_copy(glu_hbm, glu, hsem.at[0]),
        pltpu.make_async_copy(outw_hbm, outw, hsem.at[1]),
        pltpu.make_async_copy(res_hbm, res.at[k], hsem.at[2]),
        pltpu.make_async_copy(wg_hbm.at[0], wg, hsem.at[3]),
        pltpu.make_async_copy(wu_hbm.at[0], wu, hsem.at[4]),
        pltpu.make_async_copy(wd_hbm.at[0], wd, hsem.at[5]),
    ]
    for load in loads:
        load.start()

    barrier = pltpu.get_barrier_semaphore()
    pl.semaphore_signal(barrier, inc=1, device_id=(c, other), device_id_type=MESH)

    for d in (1, 2, 3):
        pl.semaphore_signal(barrier, inc=1, device_id=(c - x + (x + d) % 4, k), device_id_type=MESH)
    for d in range(1, 16):
        pl.semaphore_signal(barrier, inc=1, device_id=((c + 4 * d) % 64, k), device_id_type=MESH)

    lam_r, lam_i = lr_ref[...], li_ref[...]
    decay_re, decay_im = power(lam_r, lam_i, 1.0)
    numer_re = decay_re - 1.0
    denom = lam_r * lam_r + lam_i * lam_i
    hold_re = (numer_re * lam_r + decay_im * lam_i) / denom
    hold_im = (decay_im * lam_r - numer_re * lam_i) / denom
    hold_re = jnp.broadcast_to(hold_re[:, None, :], (32, 16, 64)).reshape(512, 64)
    hold_im = jnp.broadcast_to(hold_im[:, None, :], (32, 16, 64)).reshape(512, 64)
    drive = (
        (hold_re * in_ref[0] - hold_im * in_ref[1]).astype(BF16),
        (hold_re * in_ref[1] + hold_im * in_ref[0]).astype(BF16),
    )
    spread = (iota((64, 1024), 1) % 64 == iota((64, 1024), 0)).astype(F32).astype(BF16)
    own_block = iota((256, 1024), 0) // 16 == iota((256, 1024), 1) // 64
    row, col = iota((256, 256), 0), iota((256, 256), 1)
    order = (col == (row % SEG) * STEPS + row // SEG).astype(F32).astype(BF16)
    unorder = (row == (col % SEG) * STEPS + col // SEG).astype(F32).astype(BF16)
    ordered = dot(order, u_ref[...]).astype(BF16)
    for half in range(2):
        for part in range(2):
            block = dot(drive[part][256 * half : 256 * half + 256], spread)
            block = jnp.where(own_block, block, 0.0).astype(BF16)
            push[part, :, 1024 * half : 1024 * half + 1024] = dot(
                ordered[:, 256 * half : 256 * half + 256], block
            )

    def dense(ref):
        return jnp.concatenate([ref[pl.ds(n, 16, stride=2), :] for n in range(2)], axis=1)

    dense_r, dense_i = dense(lr_ref), dense(li_ref)
    p1 = power(dense_r, dense_i, 1.0)
    p32 = power(dense_r, dense_i, 32.0)
    p64 = power(dense_r, dense_i, 64.0)
    p128 = power(dense_r, dense_i, 128.0)
    q1 = power(dense_r, dense_i, 256.0)
    q2 = complex_mul(q1, q1)
    q3 = complex_mul(q2, q1)
    q4 = complex_mul(q2, q2)
    one = (jnp.ones_like(dense_r), jnp.zeros_like(dense_r))

    def segment_powers(j):
        def lane(v):
            return jnp.broadcast_to(lanes_of(v[4 * j : 4 * j + 4, :]), (8, 512))

        return [tuple(lane(v) for v in p) for p in (p1, p32, p64, p128)]

    seg = iota((8, 512), 0)
    for j in range(4):
        at = 512 * j
        d1, d32, d64, d128 = segment_powers(j)

        def step(i, h):
            rows = pl.ds(pl.multiple_of(i * 8, 8), 8)
            return complex_fma(d1, h, (push[0, rows, at : at + 512], push[1, rows, at : at + 512]))

        zero = jnp.zeros((8, 512), F32)
        h = lax.fori_loop(0, STEPS, step, (zero, zero), unroll=4)
        for d, p in ((1, d32), (2, d64), (4, d128)):
            moved = tuple(jnp.where(seg >= d, pltpu.roll(v, d, 0), 0.0) for v in h)
            h = complex_fma(p, moved, h)
        for part in range(2):
            edge[part, :, at : at + 512] = jnp.where(seg >= 1, pltpu.roll(h[part], 1, 0), 0.0)
            for n in range(4):
                fin[part, 4 * j + n : 4 * j + n + 1, :] = h[part][7:8, 128 * n : 128 * n + 128]

    pl.semaphore_wait(barrier, 19)

    def remote(src, dst, s, r, device):
        return pltpu.make_async_remote_copy(
            src_ref=src, dst_ref=dst, send_sem=s, recv_sem=r, device_id=device, device_id_type=MESH
        )

    along = [
        remote(fin, xbuf.at[d - 1], xs.at[d - 1], xr.at[d - 1], (c - x + (x + d) % 4, k))
        for d in (1, 2, 3)
    ]
    for copy in along:
        copy.start()
    ids_copy = remote(ids_ref, ids2, psend.at[0], precv.at[0], (c, other))
    ids_copy.start()
    rw_copy = remote(rw_ref, rw2, psend.at[4], precv.at[4], (c, other))
    rw_copy.start()
    res_copy = remote(res_hbm, res.at[k], psend.at[1], precv.at[1], (c, other))
    res_copy.start()

    for half in range(2):
        for part in range(2):
            piece = ro_ref[16 * half : 16 * half + 16, :, 64 * part : 64 * part + 64]
            piece = dot(piece.reshape(256, 64).astype(BF16), spread)
            cblk[half, :, 1024 * part : 1024 * part + 1024] = jnp.where(own_block, piece, 0.0).astype(BF16)

    for copy in along:
        copy.wait()

    def pick(n):
        return tuple(
            jnp.where(n == 0, a, jnp.where(n == 1, b, jnp.where(n == 2, e, f)))
            for a, b, e, f in zip(one, q1, q2, q3)
        )

    own = (fin[0], fin[1])
    total = complex_mul(pick(3 - x), own)
    inside = (jnp.zeros_like(dense_r), jnp.zeros_like(dense_r))
    for d in (1, 2, 3):
        theirs = (xbuf[d - 1, 0], xbuf[d - 1, 1])
        total = complex_fma(pick(3 - (x - d + 4) % 4), theirs, total)
        grown = complex_fma((one, q1, q2)[d - 1], theirs, inside)
        inside = tuple(jnp.where(d <= x, a, b) for a, b in zip(grown, inside))
    line[0] = total[0]
    line[1] = total[1]

    def to_line(target, carry):
        remote(line, ybuf.at[ln], ys.at[target], yr.at[ln], (target * 4 + x, k)).start()
        return carry

    lax.fori_loop(ln + 1, 16, to_line, 0)

    ids_copy.wait()
    rw_copy.wait()
    slot = iota((64, 128), 0)
    code = jnp.zeros((64, 128), jnp.int32)
    for n, (dz, dy, dx) in enumerate(ORDER):
        code = jnp.where(slot == n, dz * 16 + dy * 4 + dx, code)
    chip = ((z + code // 16) % 4) * 16 + ((y + code // 4 % 4) % 4) * 4 + (x + code % 4) % 4
    expert = chip * 2 + k
    before = (iota((128, 128), 0) < iota((128, 128), 1)).astype(F32).astype(BF16)
    sub = iota((64, 8, 128), 1)
    for b in range(2):
        ids = jnp.where(k == b, ids_ref[...], ids2[...])
        weights = jnp.where(k == b, rw_ref[...], rw2[...])
        first = ids[0:1, :] == expert
        second = ids[1:2, :] == expert
        named = jnp.logical_or(first, second)
        rank = dot(named.astype(F32).astype(BF16), before)
        rank = jnp.where(named, rank + 4.0 * b, -1.0)
        weight = jnp.where(first, weights[0:1, :], weights[1:2, :])
        hit = rank[:, None, :] == sub.astype(F32)
        hot[:, 128 * b : 128 * b + 128] = hit.astype(F32).reshape(512, 128).astype(BF16)
        scaled = jnp.where(hit, weight[:, None, :], 0.0).reshape(512, 128)
        scaled = scaled.T
        high = scaled.astype(BF16)
        comb[b, :, 0:512] = high
        comb[b, :, 512:1024] = (scaled - high.astype(F32)).astype(BF16)

    loads[2].wait()
    res_copy.wait()
    for n in range(4):
        cols = slice(512 * n, 512 * n + 512)
        rows = jnp.concatenate([res[0, :, cols], res[1, :, cols]], axis=0)
        send[0:EARLY_SLOTS, :, cols] = (
            dot(hot[0 : 8 * EARLY_SLOTS], rows).reshape(EARLY_SLOTS, 8, 512).astype(BF16)
        )

    def send_rows(first, last):
        for n in range(max(1, first), last):
            q = n // PER_CHUNK
            remote(send.at[n], recv.at[n], ssem.at[q], rsem.at[q], (chip_at(ORDER[n], 1), k)).start()

    def from_line(n, acc):
        remote(line, ybuf.at[n], ys.at[0], yr.at[n], (c, other)).wait_recv()
        return complex_fma(q4, acc, (ybuf[n, 0], ybuf[n, 1]))

    earlier = lax.fori_loop(0, ln, from_line, (jnp.zeros_like(dense_r), jnp.zeros_like(dense_r)))
    incoming = complex_fma(pick(x), earlier, inside)

    for j in range(4):
        at = 512 * j
        d1, d32, d64, d128 = segment_powers(j)
        to_seg = (jnp.ones((8, 512), F32), jnp.zeros((8, 512), F32))
        for bit, p in ((1, d32), (2, d64), (4, d128)):
            grown = complex_mul(to_seg, p)
            to_seg = tuple(jnp.where(seg // bit % 2 == 1, a, b) for a, b in zip(grown, to_seg))
        entering = tuple(
            jnp.broadcast_to(lanes_of(v[4 * j : 4 * j + 4, :]), (8, 512)) for v in incoming
        )
        h = complex_fma(to_seg, entering, (edge[0, :, at : at + 512], edge[1, :, at : at + 512]))
        half, base = j // 2, 512 * (j % 2)

        def double_step(i, h):
            rows = pl.ds(pl.multiple_of(i * 16, 16), 16)
            pr, pi = push[0, rows, at : at + 512], push[1, rows, at : at + 512]
            h = complex_fma(d1, h, (pr[0:8], pi[0:8]))
            g = complex_fma(d1, h, (pr[8:16], pi[8:16]))
            st[half, rows, base : base + 512] = jnp.concatenate([h[0], g[0]], axis=0).astype(BF16)
            st[half, rows, 1024 + base : 1536 + base] = jnp.concatenate(
                [h[1], g[1]], axis=0
            ).astype(BF16)
            return g

        lax.fori_loop(0, STEPS // 2, double_step, h, unroll=2)

    read = jnp.concatenate([dot_t(st[0], cblk[0]), dot_t(st[1], cblk[1])], axis=1)
    activated = jax.nn.gelu(read + skip_ref[...] * ordered.astype(F32)).astype(BF16)
    pre[k] = dot(unorder, activated).astype(BF16)
    pre_copy = remote(pre.at[k], pre.at[k], psend.at[2], precv.at[2], (c, other))
    pre_copy.start()

    send_rows(1, 16)

    loads[0].wait()
    lin = dot(pre[k], glu[pl.ds(pl.multiple_of(k * 512, 512), 512), :])
    pre_copy.wait()
    lin = lin + dot(pre[other], glu[pl.ds(pl.multiple_of(other * 512, 512), 512), :])
    full = jnp.concatenate([pre[0], pre[1]], axis=1).astype(F32)
    gated = (full * jax.nn.sigmoid(lin)).astype(BF16)
    for n in range(2):
        cols = slice(512 * n, 512 * n + 512)
        gsend[:, :, cols] = (
            dot(hot[0 : 8 * EARLY_SLOTS], gated[:, cols]).reshape(EARLY_SLOTS, 8, 512).astype(BF16)
        )
    for n in range(1, EARLY_SLOTS):
        q = n // PER_CHUNK
        remote(gsend.at[n], grecv.at[n], gsem.at[q], grsem.at[q], (chip_at(ORDER[n], 1), k)).start()
    loads[1].wait()
    squares = jnp.zeros((256, 1), F32)
    for n in range(4):
        cols = slice(512 * n, 512 * n + 512)
        start = jnp.concatenate([res[0, :, cols], res[1, :, cols]], axis=0).astype(F32)
        value = start + dot(gated, outw[:, cols])
        squares = squares + jnp.sum(value * value, axis=1, keepdims=True)
        mixed[:, cols] = value
    scale = lax.rsqrt(squares * (1.0 / 2048.0) + EPSILON)
    for n in range(4):
        cols = slice(512 * n, 512 * n + 512)
        normed[:, cols] = (mixed[:, cols] * scale * gain_ref[:, cols]).astype(BF16)
    for n in range(4):
        cols = slice(512 * n, 512 * n + 512)
        send[EARLY_SLOTS:64, :, cols] = (
            dot(hot[8 * EARLY_SLOTS : 512], normed[:, cols])
            .reshape(64 - EARLY_SLOTS, 8, 512)
            .astype(BF16)
        )

    send_rows(EARLY_SLOTS, 64)
    recv[0] = send[0]
    grecv[0] = gsend[0]
    for n in (3, 4, 5):
        loads[n].wait()

    def arrived(buffer, sem, q):
        first = 1 if q == 0 else 0
        rows = pl.ds(q * PER_CHUNK + first, PER_CHUNK - first)
        return remote(buffer.at[rows], buffer.at[rows], sem.at[q], sem.at[q], (c, other))

    for q in range(CHUNKS):
        arrived(recv, rsem, q).wait_recv()
        if q < EARLY:
            arrived(grecv, grsem, q).wait_recv()
        slots = slice(PER_CHUNK * q, PER_CHUNK * q + PER_CHUNK)
        rows_in = recv[slots].reshape(8 * PER_CHUNK, 2048)
        if q < EARLY:
            early = dot(grecv[slots].reshape(8 * PER_CHUNK, 1024), outw[...]) + rows_in.astype(F32)
            mean = jnp.sum(early * early, axis=1, keepdims=True) * (1.0 / 2048.0)
            rows_in = (early * lax.rsqrt(mean + EPSILON) * gain_ref[...]).astype(BF16)
        gate_part = dot(rows_in, wg[...])
        up_part = dot(rows_in, wu[...])
        hidden = (gate_part * jax.nn.sigmoid(gate_part) * up_part).astype(BF16)
        ans[slots] = dot(hidden, wd[...]).astype(BF16).reshape(PER_CHUNK, 8, 2048)
        for n in range(max(1, PER_CHUNK * q), PER_CHUNK * q + PER_CHUNK):
            remote(ans.at[n], ret.at[n], asem.at[q], bsem.at[q], (chip_at(ORDER[n], -1), k)).start()
        if q == 0:
            ret[0] = ans[0]

    for half in range(2):
        for q in range(half * CHUNKS // 2, (half + 1) * CHUNKS // 2):
            arrived(ret, bsem, q).wait_recv()
        returned = ret[32 * half : 32 * half + 32].reshape(256, 2048)
        high = slice(256 * half, 256 * half + 256)
        low = slice(512 + 256 * half, 768 + 256 * half)
        theirs, mine = comb[other], comb[k]
        routed = dot(theirs[:, high], returned) + dot(theirs[:, low], returned)
        if half == 0:
            part_sum[...] = routed
            own_rows = pl.ds(pl.multiple_of(k * 128, 128), 128)
            own_sum[...] = (
                mixed[own_rows, :] + dot(mine[:, high], returned) + dot(mine[:, low], returned)
            )
        else:
            part_out[...] = (part_sum[...] + routed).astype(BF16)
            part_copy = remote(part_out, part_in, psend.at[3], precv.at[3], (c, other))
            part_copy.start()
            own_sum[...] = own_sum[...] + dot(mine[:, high], returned) + dot(mine[:, low], returned)
    part_copy.wait()
    o_ref[...] = (own_sum[...] + part_in[...].astype(F32)).astype(BF16)

    def line_sent(target, carry):
        remote(line, ybuf.at[ln], ys.at[target], yr.at[ln], (target * 4 + x, k)).wait_send()
        return carry

    lax.fori_loop(ln + 1, 16, line_sent, 0)
    for q in range(CHUNKS):
        arrived(send, ssem, q).wait_send()
        if q < EARLY:
            arrived(gsend, gsem, q).wait_send()
        arrived(ans, asem, q).wait_send()


def on_device(
    ssm_input, lam_real, lam_imag, state_in, read_out, channel_skip, glu_weight, out_weight,
    residual, norm_gain, expert_ids, route_weight, expert_gate, expert_up, expert_down,
):
    vmem = pl.BlockSpec(memory_space=pltpu.VMEM)
    hbm = pl.BlockSpec(memory_space=pl.ANY)
    dma = pltpu.SemaphoreType.DMA
    return pl.pallas_call(
        body,
        out_shape=jax.ShapeDtypeStruct((128, 2048), BF16),
        in_specs=[vmem] * 9 + [hbm] * 6,
        out_specs=vmem,
        scratch_shapes=[
            pltpu.VMEM((1024, 1024), BF16),
            pltpu.VMEM((1024, 2048), BF16),
            pltpu.VMEM((2, 128, 2048), BF16),
            pltpu.VMEM((2048, 512), BF16),
            pltpu.VMEM((2048, 512), BF16),
            pltpu.VMEM((512, 2048), BF16),
            pltpu.VMEM((2, 128), jnp.int32),
            pltpu.VMEM((2, 128), F32),
            pltpu.VMEM((2, 256, 2048), F32),
            pltpu.VMEM((2, 8, 2048), F32),
            pltpu.VMEM((2, 16, 128), F32),
            pltpu.VMEM((3, 2, 16, 128), F32),
            pltpu.VMEM((16, 2, 16, 128), F32),
            pltpu.VMEM((2, 16, 128), F32),
            pltpu.VMEM((2, 256, 2048), BF16),
            pltpu.VMEM((2, 256, 2048), BF16),
            pltpu.VMEM((512, 256), BF16),
            pltpu.VMEM((2, 128, 1024), BF16),
            pltpu.VMEM((2, 256, 512), BF16),
            pltpu.VMEM((256, 2048), F32),
            pltpu.VMEM((256, 2048), BF16),
            pltpu.VMEM((64, 8, 2048), BF16),
            pltpu.VMEM((64, 8, 2048), BF16),
            pltpu.VMEM((64, 8, 2048), BF16),
            pltpu.VMEM((64, 8, 2048), BF16),
            pltpu.VMEM((128, 2048), BF16),
            pltpu.VMEM((128, 2048), BF16),
            pltpu.VMEM((128, 2048), F32),
            pltpu.VMEM((128, 2048), F32),
            pltpu.VMEM((EARLY_SLOTS, 8, 1024), BF16),
            pltpu.VMEM((EARLY_SLOTS, 8, 1024), BF16),
            dma((6,)), dma((3,)), dma((3,)), dma((16,)), dma((16,)), dma((5,)), dma((5,)),
            dma((4,)), dma((4,)), dma((4,)), dma((4,)), dma((EARLY,)), dma((EARLY,)),
        ],
        compiler_params=pltpu.CompilerParams(
            collective_id=0, has_side_effects=True, vmem_limit_bytes=60 * 1024 * 1024
        ),
    )(
        ssm_input, lam_real, lam_imag, state_in.reshape(2, 512, 64),
        read_out.transpose(0, 2, 1), channel_skip.reshape(1, 512), norm_gain.reshape(1, 2048),
        expert_ids.T, route_weight.T,
        glu_weight, out_weight, residual, expert_gate, expert_up, expert_down,
    )


def solution(mesh):
    both = P(("sp", "tp"), None)
    each = P(("sp", "tp"), None, None)
    in_specs = (
        P("sp", "tp"), P("tp", None), P("tp", None), P(None, "tp", None, None), P("tp", None, None),
        P("tp"), P(), P(), both, P(), both, both, each, each, each,
    )
    return jax.shard_map(on_device, mesh=mesh, in_specs=in_specs, out_specs=both, check_vma=False)
```

```python
import functools

import jax
import jax.numpy as jnp
from jax import lax
from jax.experimental import pallas as pl
from jax.experimental.pallas import tpu as pltpu
from jax.sharding import PartitionSpec as P

EPSILON = 1e-06
F32 = jnp.float32
BF16 = jnp.bfloat16
MESH = pl.DeviceIdType.MESH
SEG = 8
STEPS = 32
PER_CHUNK = 8
CHUNKS = 64 // PER_CHUNK
EARLY = 3
EARLY_SLOTS = EARLY * PER_CHUNK


def steps_of(shift):
    both = []
    for d in shift:
        both += [float(d == 1) + float(d == 2), float(d == 3) + float(d == 2)]
    return both


def balanced_order():
    left = [(n // 16, n // 4 % 4, n % 4) for n in range(1, 64)]
    total, order = [0.0] * 6, [(0, 0, 0)]
    while left:

        near = len(order) < EARLY_SLOTS
        limit = 2 if near else 6

        def cost(shift):
            hops = sum(steps_of(shift))
            now = [a + b for a, b in zip(total, steps_of(shift))]
            return (hops > limit, max(now) - min(now), hops if near else -hops)

        best = min(left, key=cost)
        left.remove(best)
        order.append(best)
        total = [a + b for a, b in zip(total, steps_of(best))]
    return order


ORDER = balanced_order()


def dot(a, b):
    return jnp.dot(a, b, preferred_element_type=F32)


def dot_t(a, b):
    return lax.dot_general(a, b, (((1,), (1,)), ((), ())), preferred_element_type=F32)


def iota(shape, dim):
    return lax.broadcasted_iota(jnp.int32, shape, dim)


def complex_mul(a, b):
    return a[0] * b[0] - a[1] * b[1], a[0] * b[1] + a[1] * b[0]


def complex_fma(a, b, c):
    return a[0] * b[0] - a[1] * b[1] + c[0], a[0] * b[1] + a[1] * b[0] + c[1]


def power(lam_real, lam_imag, exponent):
    magnitude = jnp.exp(exponent * lam_real)
    angle = exponent * lam_imag
    turns = jnp.floor(angle * 0.15915494309189535 + 0.5)
    angle = (angle - turns * 6.28125) - turns * 0.0019353071795864769
    return magnitude * jnp.cos(angle), magnitude * jnp.sin(angle)


def lanes_of(rows):
    return jnp.concatenate([rows[i : i + 1, :] for i in range(rows.shape[0])], axis=1)


def body(
    u_ref, lr_ref, li_ref, in_ref, ro_ref, skip_ref, gain_ref, ids_ref, rw_ref,
    glu_hbm, outw_hbm, res_hbm, wg_hbm, wu_hbm, wd_hbm,
    o_ref,
    glu, outw, res, wg, wu, wd, ids2, rw2,
    push, edge, fin, xbuf, ybuf, line, st, cblk, hot, comb,
    pre, mixed, normed, send, recv, ans, ret, part_out, part_in, part_sum, own_sum, gsend, grecv,
    hsem, xs, xr, ys, yr, psend, precv, ssem, rsem, asem, bsem, gsem, grsem,
):
    c = lax.axis_index("sp")
    k = lax.axis_index("tp")
    other = 1 - k
    z, y, x = c // 16, (c // 4) % 4, c % 4
    ln = c // 4

    def chip_at(shift, sign):
        dz, dy, dx = (sign * d % 4 for d in shift)
        return ((z + dz) % 4) * 16 + ((y + dy) % 4) * 4 + (x + dx) % 4

    loads = [
        pltpu.make_async_copy(glu_hbm, glu, hsem.at[0]),
        pltpu.make_async_copy(outw_hbm, outw, hsem.at[1]),
        pltpu.make_async_copy(res_hbm, res.at[k], hsem.at[2]),
        pltpu.make_async_copy(wg_hbm.at[0], wg, hsem.at[3]),
        pltpu.make_async_copy(wu_hbm.at[0], wu, hsem.at[4]),
        pltpu.make_async_copy(wd_hbm.at[0], wd, hsem.at[5]),
    ]
    for load in loads:
        load.start()

    barrier = pltpu.get_barrier_semaphore()
    pl.semaphore_signal(barrier, inc=1, device_id=(c, other), device_id_type=MESH)

    for d in (1, 2, 3):
        pl.semaphore_signal(barrier, inc=1, device_id=(c - x + (x + d) % 4, k), device_id_type=MESH)
    for d in range(1, 16):
        pl.semaphore_signal(barrier, inc=1, device_id=((c + 4 * d) % 64, k), device_id_type=MESH)

    lam_r, lam_i = lr_ref[...], li_ref[...]
    decay_re, decay_im = power(lam_r, lam_i, 1.0)
    numer_re = decay_re - 1.0
    denom = lam_r * lam_r + lam_i * lam_i
    hold_re = (numer_re * lam_r + decay_im * lam_i) / denom
    hold_im = (decay_im * lam_r - numer_re * lam_i) / denom
    hold_re = jnp.broadcast_to(hold_re[:, None, :], (32, 16, 64)).reshape(512, 64)
    hold_im = jnp.broadcast_to(hold_im[:, None, :], (32, 16, 64)).reshape(512, 64)
    drive = (
        (hold_re * in_ref[0] - hold_im * in_ref[1]).astype(BF16),
        (hold_re * in_ref[1] + hold_im * in_ref[0]).astype(BF16),
    )
    spread = (iota((64, 1024), 1) % 64 == iota((64, 1024), 0)).astype(F32).astype(BF16)
    own_block = iota((256, 1024), 0) // 16 == iota((256, 1024), 1) // 64
    row, col = iota((256, 256), 0), iota((256, 256), 1)
    order = (col == (row % SEG) * STEPS + row // SEG).astype(F32).astype(BF16)
    unorder = (row == (col % SEG) * STEPS + col // SEG).astype(F32).astype(BF16)
    ordered = dot(order, u_ref[...]).astype(BF16)
    for half in range(2):
        for part in range(2):
            block = dot(drive[part][256 * half : 256 * half + 256], spread)
            block = jnp.where(own_block, block, 0.0).astype(BF16)
            push[part, :, 1024 * half : 1024 * half + 1024] = dot(
                ordered[:, 256 * half : 256 * half + 256], block
            )

    def dense(ref):
        return jnp.concatenate([ref[pl.ds(n, 16, stride=2), :] for n in range(2)], axis=1)

    dense_r, dense_i = dense(lr_ref), dense(li_ref)
    p1 = power(dense_r, dense_i, 1.0)
    p32 = power(dense_r, dense_i, 32.0)
    p64 = power(dense_r, dense_i, 64.0)
    p128 = power(dense_r, dense_i, 128.0)
    q1 = power(dense_r, dense_i, 256.0)
    q2 = complex_mul(q1, q1)
    q3 = complex_mul(q2, q1)
    q4 = complex_mul(q2, q2)
    one = (jnp.ones_like(dense_r), jnp.zeros_like(dense_r))

    def segment_powers(j):
        def lane(v):
            return jnp.broadcast_to(lanes_of(v[4 * j : 4 * j + 4, :]), (8, 512))

        return [tuple(lane(v) for v in p) for p in (p1, p32, p64, p128)]

    seg = iota((8, 512), 0)
    for j in range(4):
        at = 512 * j
        d1, d32, d64, d128 = segment_powers(j)

        def step(i, h):
            rows = pl.ds(pl.multiple_of(i * 8, 8), 8)
            return complex_fma(d1, h, (push[0, rows, at : at + 512], push[1, rows, at : at + 512]))

        zero = jnp.zeros((8, 512), F32)
        h = lax.fori_loop(0, STEPS, step, (zero, zero), unroll=4)
        for d, p in ((1, d32), (2, d64), (4, d128)):
            moved = tuple(jnp.where(seg >= d, pltpu.roll(v, d, 0), 0.0) for v in h)
            h = complex_fma(p, moved, h)
        for part in range(2):
            edge[part, :, at : at + 512] = jnp.where(seg >= 1, pltpu.roll(h[part], 1, 0), 0.0)
            for n in range(4):
                fin[part, 4 * j + n : 4 * j + n + 1, :] = h[part][7:8, 128 * n : 128 * n + 128]

    pl.semaphore_wait(barrier, 19)

    def remote(src, dst, s, r, device):
        return pltpu.make_async_remote_copy(
            src_ref=src, dst_ref=dst, send_sem=s, recv_sem=r, device_id=device, device_id_type=MESH
        )

    along = [
        remote(fin, xbuf.at[d - 1], xs.at[d - 1], xr.at[d - 1], (c - x + (x + d) % 4, k))
        for d in (1, 2, 3)
    ]
    for copy in along:
        copy.start()
    ids_copy = remote(ids_ref, ids2, psend.at[0], precv.at[0], (c, other))
    ids_copy.start()
    rw_copy = remote(rw_ref, rw2, psend.at[4], precv.at[4], (c, other))
    rw_copy.start()
    res_copy = remote(res_hbm, res.at[k], psend.at[1], precv.at[1], (c, other))
    res_copy.start()

    for half in range(2):
        for part in range(2):
            piece = ro_ref[16 * half : 16 * half + 16, :, 64 * part : 64 * part + 64]
            piece = dot(piece.reshape(256, 64).astype(BF16), spread)
            cblk[half, :, 1024 * part : 1024 * part + 1024] = jnp.where(own_block, piece, 0.0).astype(BF16)

    for copy in along:
        copy.wait()

    def pick(n):
        return tuple(
            jnp.where(n == 0, a, jnp.where(n == 1, b, jnp.where(n == 2, e, f)))
            for a, b, e, f in zip(one, q1, q2, q3)
        )

    own = (fin[0], fin[1])
    total = complex_mul(pick(3 - x), own)
    inside = (jnp.zeros_like(dense_r), jnp.zeros_like(dense_r))
    for d in (1, 2, 3):
        theirs = (xbuf[d - 1, 0], xbuf[d - 1, 1])
        total = complex_fma(pick(3 - (x - d + 4) % 4), theirs, total)
        grown = complex_fma((one, q1, q2)[d - 1], theirs, inside)
        inside = tuple(jnp.where(d <= x, a, b) for a, b in zip(grown, inside))
    line[0] = total[0]
    line[1] = total[1]

    def to_line(target, carry):
        remote(line, ybuf.at[ln], ys.at[target], yr.at[ln], (target * 4 + x, k)).start()
        return carry

    lax.fori_loop(ln + 1, 16, to_line, 0)

    ids_copy.wait()
    rw_copy.wait()
    slot = iota((64, 128), 0)
    code = jnp.zeros((64, 128), jnp.int32)
    for n, (dz, dy, dx) in enumerate(ORDER):
        code = jnp.where(slot == n, dz * 16 + dy * 4 + dx, code)
    chip = ((z + code // 16) % 4) * 16 + ((y + code // 4 % 4) % 4) * 4 + (x + code % 4) % 4
    expert = chip * 2 + k
    before = (iota((128, 128), 0) < iota((128, 128), 1)).astype(F32).astype(BF16)
    sub = iota((64, 8, 128), 1)
    for b in range(2):
        ids = jnp.where(k == b, ids_ref[...], ids2[...])
        weights = jnp.where(k == b, rw_ref[...], rw2[...])
        first = ids[0:1, :] == expert
        second = ids[1:2, :] == expert
        named = jnp.logical_or(first, second)
        rank = dot(named.astype(F32).astype(BF16), before)
        rank = jnp.where(named, rank + 4.0 * b, -1.0)
        weight = jnp.where(first, weights[0:1, :], weights[1:2, :])
        hit = rank[:, None, :] == sub.astype(F32)
        hot[:, 128 * b : 128 * b + 128] = hit.astype(F32).reshape(512, 128).astype(BF16)
        scaled = jnp.where(hit, weight[:, None, :], 0.0).reshape(512, 128)
        scaled = scaled.T
        high = scaled.astype(BF16)
        comb[b, :, 0:512] = high
        comb[b, :, 512:1024] = (scaled - high.astype(F32)).astype(BF16)

    loads[2].wait()
    res_copy.wait()
    for n in range(4):
        cols = slice(512 * n, 512 * n + 512)
        rows = jnp.concatenate([res[0, :, cols], res[1, :, cols]], axis=0)
        send[0:EARLY_SLOTS, :, cols] = (
            dot(hot[0 : 8 * EARLY_SLOTS], rows).reshape(EARLY_SLOTS, 8, 512).astype(BF16)
        )

    def send_rows(first, last):
        for n in range(max(1, first), last):
            q = n // PER_CHUNK
            remote(send.at[n], recv.at[n], ssem.at[q], rsem.at[q], (chip_at(ORDER[n], 1), k)).start()

    def from_line(n, acc):
        remote(line, ybuf.at[n], ys.at[0], yr.at[n], (c, other)).wait_recv()
        return complex_fma(q4, acc, (ybuf[n, 0], ybuf[n, 1]))

    earlier = lax.fori_loop(0, ln, from_line, (jnp.zeros_like(dense_r), jnp.zeros_like(dense_r)))
    incoming = complex_fma(pick(x), earlier, inside)

    for j in range(4):
        at = 512 * j
        d1, d32, d64, d128 = segment_powers(j)
        to_seg = (jnp.ones((8, 512), F32), jnp.zeros((8, 512), F32))
        for bit, p in ((1, d32), (2, d64), (4, d128)):
            grown = complex_mul(to_seg, p)
            to_seg = tuple(jnp.where(seg // bit % 2 == 1, a, b) for a, b in zip(grown, to_seg))
        entering = tuple(
            jnp.broadcast_to(lanes_of(v[4 * j : 4 * j + 4, :]), (8, 512)) for v in incoming
        )
        h = complex_fma(to_seg, entering, (edge[0, :, at : at + 512], edge[1, :, at : at + 512]))
        half, base = j // 2, 512 * (j % 2)

        def double_step(i, h):
            rows = pl.ds(pl.multiple_of(i * 16, 16), 16)
            pr, pi = push[0, rows, at : at + 512], push[1, rows, at : at + 512]
            h = complex_fma(d1, h, (pr[0:8], pi[0:8]))
            g = complex_fma(d1, h, (pr[8:16], pi[8:16]))
            st[half, rows, base : base + 512] = jnp.concatenate([h[0], g[0]], axis=0).astype(BF16)
            st[half, rows, 1024 + base : 1536 + base] = jnp.concatenate(
                [h[1], g[1]], axis=0
            ).astype(BF16)
            return g

        lax.fori_loop(0, STEPS // 2, double_step, h, unroll=2)

    read = jnp.concatenate([dot_t(st[0], cblk[0]), dot_t(st[1], cblk[1])], axis=1)
    activated = jax.nn.gelu(read + skip_ref[...] * ordered.astype(F32)).astype(BF16)
    pre[k] = dot(unorder, activated).astype(BF16)
    pre_copy = remote(pre.at[k], pre.at[k], psend.at[2], precv.at[2], (c, other))
    pre_copy.start()

    send_rows(1, EARLY_SLOTS)

    loads[0].wait()
    lin = dot(pre[k], glu[pl.ds(pl.multiple_of(k * 512, 512), 512), :])
    pre_copy.wait()
    lin = lin + dot(pre[other], glu[pl.ds(pl.multiple_of(other * 512, 512), 512), :])
    full = jnp.concatenate([pre[0], pre[1]], axis=1).astype(F32)
    gated = (full * jax.nn.sigmoid(lin)).astype(BF16)
    for n in range(2):
        cols = slice(512 * n, 512 * n + 512)
        gsend[:, :, cols] = (
            dot(hot[0 : 8 * EARLY_SLOTS], gated[:, cols]).reshape(EARLY_SLOTS, 8, 512).astype(BF16)
        )
    for n in range(1, EARLY_SLOTS):
        q = n // PER_CHUNK
        remote(gsend.at[n], grecv.at[n], gsem.at[q], grsem.at[q], (chip_at(ORDER[n], 1), k)).start()
    loads[1].wait()
    squares = jnp.zeros((256, 1), F32)
    for n in range(4):
        cols = slice(512 * n, 512 * n + 512)
        start = jnp.concatenate([res[0, :, cols], res[1, :, cols]], axis=0).astype(F32)
        value = start + dot(gated, outw[:, cols])
        squares = squares + jnp.sum(value * value, axis=1, keepdims=True)
        mixed[:, cols] = value
    scale = lax.rsqrt(squares * (1.0 / 2048.0) + EPSILON)
    for n in range(4):
        cols = slice(512 * n, 512 * n + 512)
        normed[:, cols] = (mixed[:, cols] * scale * gain_ref[:, cols]).astype(BF16)
    for n in range(4):
        cols = slice(512 * n, 512 * n + 512)
        send[EARLY_SLOTS:64, :, cols] = (
            dot(hot[8 * EARLY_SLOTS : 512], normed[:, cols])
            .reshape(64 - EARLY_SLOTS, 8, 512)
            .astype(BF16)
        )

    send_rows(EARLY_SLOTS, 64)
    recv[0] = send[0]
    grecv[0] = gsend[0]
    for n in (3, 4, 5):
        loads[n].wait()

    def arrived(buffer, sem, q):
        first = 1 if q == 0 else 0
        rows = pl.ds(q * PER_CHUNK + first, PER_CHUNK - first)
        return remote(buffer.at[rows], buffer.at[rows], sem.at[q], sem.at[q], (c, other))

    for q in range(CHUNKS):
        arrived(recv, rsem, q).wait_recv()
        if q < EARLY:
            arrived(grecv, grsem, q).wait_recv()
        slots = slice(PER_CHUNK * q, PER_CHUNK * q + PER_CHUNK)
        rows_in = recv[slots].reshape(8 * PER_CHUNK, 2048)
        if q < EARLY:
            early = dot(grecv[slots].reshape(8 * PER_CHUNK, 1024), outw[...]) + rows_in.astype(F32)
            mean = jnp.sum(early * early, axis=1, keepdims=True) * (1.0 / 2048.0)
            rows_in = (early * lax.rsqrt(mean + EPSILON) * gain_ref[...]).astype(BF16)
        gate_part = dot(rows_in, wg[...])
        up_part = dot(rows_in, wu[...])
        hidden = (gate_part * jax.nn.sigmoid(gate_part) * up_part).astype(BF16)
        ans[slots] = dot(hidden, wd[...]).astype(BF16).reshape(PER_CHUNK, 8, 2048)
        for n in range(max(1, PER_CHUNK * q), PER_CHUNK * q + PER_CHUNK):
            remote(ans.at[n], ret.at[n], asem.at[q], bsem.at[q], (chip_at(ORDER[n], -1), k)).start()
        if q == 0:
            ret[0] = ans[0]

    for q in range(CHUNKS - 1):
        arrived(ret, bsem, q).wait_recv()
    last = 512 - 8 * PER_CHUNK
    theirs, mine = comb[other], comb[k]
    returned = ret[0 : 64 - PER_CHUNK].reshape(last, 2048)
    own_rows = pl.ds(pl.multiple_of(k * 128, 128), 128)
    part_sum[...] = dot(theirs[:, 0:last], returned) + dot(theirs[:, 512 : 512 + last], returned)
    own_sum[...] = (
        mixed[own_rows, :]
        + dot(mine[:, 0:last], returned)
        + dot(mine[:, 512 : 512 + last], returned)
    )
    theirs = jnp.concatenate([theirs[:, last:512], theirs[:, 512 + last : 1024]], axis=1)
    mine = jnp.concatenate([mine[:, last:512], mine[:, 512 + last : 1024]], axis=1)
    arrived(ret, bsem, CHUNKS - 1).wait_recv()
    pieces = []
    for n in range(4):
        cols = slice(512 * n, 512 * n + 512)
        tail = ret[64 - PER_CHUNK : 64, :, cols].reshape(8 * PER_CHUNK, 512)
        tail = jnp.concatenate([tail, tail], axis=0)
        part_out[n] = (part_sum[:, cols] + dot(theirs, tail)).astype(BF16)
        pieces.append(
            remote(part_out.at[n], part_in.at[n], psend.at[5 + n], precv.at[5 + n], (c, other))
        )
        pieces[n].start()
    for n in range(4):
        cols = slice(512 * n, 512 * n + 512)
        tail = ret[64 - PER_CHUNK : 64, :, cols].reshape(8 * PER_CHUNK, 512)
        tail = jnp.concatenate([tail, tail], axis=0)
        own_sum[:, cols] = own_sum[:, cols] + dot(mine, tail)
    for n in range(4):
        cols = slice(512 * n, 512 * n + 512)
        pieces[n].wait()
        o_ref[:, cols] = (own_sum[:, cols] + part_in[n].astype(F32)).astype(BF16)

    def line_sent(target, carry):
        remote(line, ybuf.at[ln], ys.at[target], yr.at[ln], (target * 4 + x, k)).wait_send()
        return carry

    lax.fori_loop(ln + 1, 16, line_sent, 0)
    for q in range(CHUNKS):
        arrived(send, ssem, q).wait_send()
        if q < EARLY:
            arrived(gsend, gsem, q).wait_send()
        arrived(ans, asem, q).wait_send()


def on_device(
    ssm_input, lam_real, lam_imag, state_in, read_out, channel_skip, glu_weight, out_weight,
    residual, norm_gain, expert_ids, route_weight, expert_gate, expert_up, expert_down,
):
    vmem = pl.BlockSpec(memory_space=pltpu.VMEM)
    hbm = pl.BlockSpec(memory_space=pl.ANY)
    dma = pltpu.SemaphoreType.DMA
    return pl.pallas_call(
        body,
        out_shape=jax.ShapeDtypeStruct((128, 2048), BF16),
        in_specs=[vmem] * 9 + [hbm] * 6,
        out_specs=vmem,
        scratch_shapes=[
            pltpu.VMEM((1024, 1024), BF16),
            pltpu.VMEM((1024, 2048), BF16),
            pltpu.VMEM((2, 128, 2048), BF16),
            pltpu.VMEM((2048, 512), BF16),
            pltpu.VMEM((2048, 512), BF16),
            pltpu.VMEM((512, 2048), BF16),
            pltpu.VMEM((2, 128), jnp.int32),
            pltpu.VMEM((2, 128), F32),
            pltpu.VMEM((2, 256, 2048), F32),
            pltpu.VMEM((2, 8, 2048), F32),
            pltpu.VMEM((2, 16, 128), F32),
            pltpu.VMEM((3, 2, 16, 128), F32),
            pltpu.VMEM((16, 2, 16, 128), F32),
            pltpu.VMEM((2, 16, 128), F32),
            pltpu.VMEM((2, 256, 2048), BF16),
            pltpu.VMEM((2, 256, 2048), BF16),
            pltpu.VMEM((512, 256), BF16),
            pltpu.VMEM((2, 128, 1024), BF16),
            pltpu.VMEM((2, 256, 512), BF16),
            pltpu.VMEM((256, 2048), F32),
            pltpu.VMEM((256, 2048), BF16),
            pltpu.VMEM((64, 8, 2048), BF16),
            pltpu.VMEM((64, 8, 2048), BF16),
            pltpu.VMEM((64, 8, 2048), BF16),
            pltpu.VMEM((64, 8, 2048), BF16),
            pltpu.VMEM((4, 128, 512), BF16),
            pltpu.VMEM((4, 128, 512), BF16),
            pltpu.VMEM((128, 2048), F32),
            pltpu.VMEM((128, 2048), F32),
            pltpu.VMEM((EARLY_SLOTS, 8, 1024), BF16),
            pltpu.VMEM((EARLY_SLOTS, 8, 1024), BF16),
            dma((6,)), dma((3,)), dma((3,)), dma((16,)), dma((16,)), dma((9,)), dma((9,)),
            dma((CHUNKS,)), dma((CHUNKS,)), dma((CHUNKS,)), dma((CHUNKS,)), dma((EARLY,)), dma((EARLY,)),
        ],
        compiler_params=pltpu.CompilerParams(
            collective_id=0, has_side_effects=True, vmem_limit_bytes=60 * 1024 * 1024
        ),
    )(
        ssm_input, lam_real, lam_imag, state_in.reshape(2, 512, 64),
        read_out.transpose(0, 2, 1), channel_skip.reshape(1, 512), norm_gain.reshape(1, 2048),
        expert_ids.T, route_weight.T,
        glu_weight, out_weight, residual, expert_gate, expert_up, expert_down,
    )


def solution(mesh):
    both = P(("sp", "tp"), None)
    each = P(("sp", "tp"), None, None)
    in_specs = (
        P("sp", "tp"), P("tp", None), P("tp", None), P(None, "tp", None, None), P("tp", None, None),
        P("tp"), P(), P(), both, P(), both, both, each, each, each,
    )
    return jax.shard_map(on_device, mesh=mesh, in_specs=in_specs, out_specs=both, check_vma=False)
```
